128 devices in a mesh: sp: 16 (over z, y), tp: 8 (over x, core).
Axes of the slice: x: 4, y: 4, z: 4, core: 2. Of those that a mesh axis runs over, the one named last changes fastest.
Arguments:
- latents: bfloat16 [4096, 4096], P('sp'), may hold values from -0.4375 to 0.4375
- query_heads: bfloat16 [4096, 16, 128], P('sp', 'tp'), may hold values from -8 to 8
- key_heads: bfloat16 [4096, 16, 128], P('sp', 'tp'), may hold values from -8 to 8
- value_heads: bfloat16 [4096, 16, 128], P('sp', 'tp'), may hold values from -6 to 6
- map_outputs: bfloat16 [4096, 2, 16, 128], P('sp', None, 'tp'), may hold values from -6 to 6
- log_sums: float32 [4096, 16, 2], P('sp', 'tp'), may hold values from -600 to 600, as said below
- out_grad: bfloat16 [4096, 16, 128], P('sp', 'tp'), may hold values from -6 to 6
- mix_lambda: float32 [16], P('tp'), may hold values from 0.3 to 0.8
- norm_gain: float32 [128], replicated, may hold values from 0.1 to 1.9
Outputs:
- query_grad: bfloat16 [4096, 16, 128], P('sp', 'tp')
- key_grad: bfloat16 [4096, 16, 128], P('sp', 'tp')
- value_grad: bfloat16 [4096, 16, 128], P('sp', 'tp')
- weight_grad: float32 [4096, 2048], P('sp', 'tp')
The draws below stay inside these ranges and needn't reach their ends.
Inputs may be any that keep to these rules, and one draw needn't show every extreme that they name: query_heads, key_heads and value_heads together with map_outputs and log_sums are one consistent causal forward pass: log_sums is the row's log-sum of exp(score_m) over keys at or before the row, and map_outputs[:, m] is prob_m times value_heads rounded to bfloat16.
All inputs are finite; a program needn't handle non-finite values.
Results may differ from the reference program's by a relative error of at most 0.019.
Values may be sent and summed in bfloat16 or wider, within the bound.
A program may use at most 64 MiB of HBM per device.

```python
import math
import jax
import jax.numpy as jnp
from jax import lax

D = 4096
HEADS = 16
DH = 64
TOKENS = 4096


def attention_forward(key):
    shape = (TOKENS, HEADS, 2 * DH)
    query_f = jnp.clip(1.3 * jax.random.normal(jax.random.fold_in(key, 101), shape, jnp.float32), -8.0, 8.0)
    key_f = jnp.clip(1.3 * jax.random.normal(jax.random.fold_in(key, 102), shape, jnp.float32), -8.0, 8.0)
    value_f = jnp.clip(jax.random.normal(jax.random.fold_in(key, 103), shape, jnp.float32), -6.0, 6.0)
    query_low = query_f.astype(jnp.bfloat16)
    key_low = key_f.astype(jnp.bfloat16)
    value_low = value_f.astype(jnp.bfloat16)
    length = TOKENS
    span = math.gcd(length, 512)
    score_scale = DH ** (-0.5)

    def per_head(inputs):
        query_one, key_one, value_one = inputs
        query_split = query_one.astype(jnp.float32).reshape(length, 2, DH)
        key_split = key_one.astype(jnp.float32).reshape(length, 2, DH)
        value_wide = value_one.astype(jnp.float32)
        key_pos = jnp.arange(length, dtype=jnp.int32)

        def visit(block_index):
            anchor = (block_index * span).astype(jnp.int32)
            query_blk = lax.dynamic_slice_in_dim(query_split, anchor, span, 0)
            scores = jnp.einsum('qmd,kmd->mqk', query_blk, key_split) * score_scale
            query_pos = anchor + jnp.arange(span, dtype=jnp.int32)
            causal = key_pos[None, :] <= query_pos[:, None]
            masked = jnp.where(causal[None], scores, -jnp.inf)
            highest = jnp.max(masked, axis=-1, keepdims=True)
            log_total = highest + jnp.log(jnp.sum(jnp.exp(masked - highest), axis=-1, keepdims=True))
            probs = jnp.exp(masked - log_total)
            outputs = jnp.einsum('mqk,ke->mqe', probs, value_wide)
            return (log_total[..., 0].T, outputs)
        lse_blocks, out_blocks = lax.map(visit, jnp.arange(length // span, dtype=jnp.int32))
        lse_head = lse_blocks.reshape(length, 2)
        out_head = jnp.transpose(out_blocks, (1, 0, 2, 3)).reshape(2, length, 2 * DH)
        return (lse_head, out_head)
    lse_all, out_all = lax.map(per_head, (jnp.transpose(query_low, (1, 0, 2)), jnp.transpose(key_low, (1, 0, 2)), jnp.transpose(value_low, (1, 0, 2))))
    log_table = jnp.transpose(lse_all, (1, 0, 2))
    out_table = jnp.transpose(out_all, (2, 1, 0, 3)).astype(jnp.bfloat16)
    return (query_low, key_low, value_low, out_table, log_table)


def draw_query_heads(key, part):
    return attention_forward(key)[0]


def draw_key_heads(key, part):
    return attention_forward(key)[1]


def draw_value_heads(key, part):
    return attention_forward(key)[2]


def draw_map_outputs(key, part):
    return attention_forward(key)[3]


def draw_log_sums(key, part):
    return attention_forward(key)[4]


def raised(values, stream_key, source, target, parts, factor):
    def block_of(position):
        return (jnp.arange(values.shape[position]) // (values.shape[position] // parts)).reshape((-1,) + (1,) * (values.ndim - 1 - position))

    near = jax.random.permutation(stream_key, parts)[block_of(target)]
    far = (block_of(target) + parts // 2) % parts
    return jnp.where((block_of(source) == near) | (block_of(source) == far), factor * values, values)


def level_of(key, extent, split, least, top_value):
    factor_of, own = 1.0, jax.random.fold_in(key, 6)
    for position, shards_of in split:
        steps = jnp.exp(jax.random.uniform(jax.random.fold_in(own, position), (shards_of,), jnp.float32, least / len(split), top_value / len(split)))
        factor_of = factor_of * jnp.repeat(steps, extent[position] // shards_of).reshape([-1 if axis == position else 1 for axis in range(len(extent))])
    return factor_of


def noise(key, dims, scale, most, pieces=(), kind=jnp.bfloat16):
    level = level_of(key, dims, pieces, -0.22, 0.18) if pieces else 1.0
    values = jax.random.normal(key, dims, jnp.float32) * scale * level
    return jnp.minimum(jnp.maximum(values, -most), most).astype(kind)


def gaussian_with(stream_key, shape, deviation, reach, shards, heavy, kind=jnp.bfloat16):
    entries = deviation * jax.random.normal(stream_key, shape, jnp.float32)
    if shards:
        entries = entries * level_of(stream_key, shape, shards, -0.22, 0.18)
    return jnp.clip(raised(entries, jax.random.fold_in(stream_key, 3), *heavy), -reach, reach).astype(kind)


def setup_inputs(seed: int = 0) -> dict:
    seeds = jax.random.split(jax.random.key(seed), 10)
    return {
        "latents": gaussian_with(seeds[0], (TOKENS, D), 0.02, 0.4375, ((0, 16),), (0, 1, 16, 2.0)),
        "query_heads": draw_query_heads(jax.random.fold_in(seeds[9], 71), 0),
        "key_heads": draw_key_heads(jax.random.fold_in(seeds[9], 71), 0),
        "value_heads": draw_value_heads(jax.random.fold_in(seeds[9], 71), 0),
        "map_outputs": draw_map_outputs(jax.random.fold_in(seeds[9], 71), 0),
        "log_sums": draw_log_sums(jax.random.fold_in(seeds[9], 71), 0),
        "out_grad": noise(seeds[6], (TOKENS, HEADS, 2 * DH), 1.0, 6.0, ((0, 16), (1, 8))),
        "mix_lambda": jnp.clip(0.3 + 0.5 * jax.random.uniform(seeds[7], (HEADS,), jnp.float32) ** level_of(seeds[7], (HEADS,), ((0, 8),), -0.2, 0.2), 0.3, 0.8),
        "norm_gain": jnp.clip(1.0 + 0.18 * jax.random.normal(seeds[8], (2 * DH,), jnp.float32), 0.1, 1.9),
    }


EPSILON = 1e-05

def reference(latents, query_heads, key_heads, value_heads, map_outputs, log_sums, out_grad, mix_lambda, norm_gain):
    highest = lax.Precision.HIGHEST
    score_scale = DH ** (-0.5)
    first_map = map_outputs[:, 0].astype(jnp.float32)
    second_map = map_outputs[:, 1].astype(jnp.float32)
    lambda_col = mix_lambda[None, :, None]
    combined = first_map - lambda_col * second_map
    inverse = lax.rsqrt(lax.optimization_barrier(jnp.mean(combined * combined, axis=-1, keepdims=True)) + EPSILON)
    weighted = norm_gain[None, None, :] * out_grad.astype(jnp.float32)
    grad_out = (inverse * weighted - inverse ** 3 * combined * lax.optimization_barrier(jnp.mean(combined * weighted, axis=-1, keepdims=True))).astype(jnp.bfloat16)
    grad_wide = lax.optimization_barrier(grad_out).astype(jnp.float32)
    row_terms = jnp.stack([lax.optimization_barrier(jnp.sum(grad_wide * first_map, axis=-1)), lax.optimization_barrier(jnp.sum(grad_wide * second_map, axis=-1))], axis=-1)
    length = query_heads.shape[0]
    span = math.gcd(length, 512)

    def per_head(inputs):
        query_one, key_one, value_one, grad_one, lse_one, term_one, lam = inputs
        query_split = query_one.astype(jnp.float32).reshape(length, 2, DH)
        key_split = key_one.astype(jnp.float32).reshape(length, 2, DH)
        value_wide = value_one.astype(jnp.float32)
        grad_full = grad_one.astype(jnp.float32)
        key_pos = jnp.arange(length, dtype=jnp.int32)
        map_signs = jnp.stack([jnp.ones((), jnp.float32), -lam])

        def visit(running, block_index):
            key_acc, value_acc = running
            anchor = (block_index * span).astype(jnp.int32)
            query_blk = lax.dynamic_slice_in_dim(query_split, anchor, span, 0)
            grad_blk = lax.dynamic_slice_in_dim(grad_full, anchor, span, 0)
            lse_blk = lax.dynamic_slice_in_dim(lse_one, anchor, span, 0)
            term_blk = lax.dynamic_slice_in_dim(term_one, anchor, span, 0)
            scores = jnp.einsum('qmd,kmd->mqk', query_blk, key_split, precision=highest) * score_scale
            query_pos = anchor + jnp.arange(span, dtype=jnp.int32)
            causal = key_pos[None, :] <= query_pos[:, None]
            softmax_maps = jnp.exp(jnp.where(causal[None], scores - lse_blk.T[:, :, None], -jnp.inf))
            mixed_grad = jnp.dot(grad_blk, value_wide.T, precision=highest)
            score_grad = map_signs[:, None, None] * softmax_maps * (mixed_grad[None] - term_blk.T[:, :, None])
            score_low = lax.optimization_barrier(score_grad.astype(jnp.bfloat16)).astype(jnp.float32)
            diff_weights = lax.optimization_barrier((softmax_maps[0] - lam * softmax_maps[1]).astype(jnp.bfloat16)).astype(jnp.float32)
            value_acc = value_acc + jnp.dot(diff_weights.T, grad_blk, precision=highest)
            query_part = score_scale * jnp.einsum('mqk,kmd->qmd', score_low, key_split, precision=highest)
            key_acc = key_acc + score_scale * jnp.einsum('mqk,qmd->kmd', score_low, query_blk, precision=highest)
            return ((key_acc, value_acc), query_part)
        start_state = (jnp.zeros((length, 2, DH), jnp.float32), jnp.zeros((length, 2 * DH), jnp.float32))
        (key_acc, value_acc), query_parts = lax.scan(visit, start_state, jnp.arange(length // span, dtype=jnp.int32))
        return (query_parts.reshape(length, 2 * DH), key_acc.reshape(length, 2 * DH), value_acc)

    def head_major(array):
        return jnp.transpose(array, (1, 0, 2))
    query_all, key_all, value_all = lax.map(per_head, (head_major(query_heads), head_major(key_heads), head_major(value_heads), head_major(grad_out), head_major(log_sums), head_major(row_terms), mix_lambda))
    query_grad = head_major(query_all).astype(jnp.bfloat16)
    key_grad = head_major(key_all).astype(jnp.bfloat16)
    value_grad = head_major(value_all).astype(jnp.bfloat16)
    weight_grad = jnp.dot(latents.T, query_grad.reshape(length, -1), preferred_element_type=jnp.float32)
    return (query_grad, key_grad, value_grad, weight_grad)
```

```python
import functools

import jax
import jax.numpy as jnp
from jax import lax
from jax.experimental import pallas as pl
from jax.experimental.pallas import tpu as pltpu
from jax.sharding import PartitionSpec as P

F32 = jnp.float32
BF16 = jnp.bfloat16
EPSILON = 1e-05
LOG2E = 1.4426950408889634
SCALE = 0.125
T = 256
W = 128
NT = (((1,), (1,)), ((), ()))


def dot(a, b):
    return jnp.dot(a, b, preferred_element_type=F32)


def dot_nt(a, b):
    return lax.dot_general(a, b, NT, preferred_element_type=F32)


def kernel(
    q_ref, k_ref, v_ref, mo_ref, lse_ref, og_ref, lam_ref, gain_ref, lat_hbm,
    qg_ref, kg_ref, vg_ref, wg_ref,
    lat, qdo, kv, st, dqt, dkv, wide, wide2, dqf,
    qtx, qrx, ktx, krx, atx, arx, btx, brx,
    lat_sem, gs, gr, rs, rr,
):
    sp = lax.axis_index("sp")
    tp = lax.axis_index("tp")
    z = sp // 4
    y = sp % 4
    pos = (y, z)

    def ring(axis, step):
        moved = lax.rem(pos[axis] + step + 4, 4)
        return moved

    def peer(axis, step):
        moved = ring(axis, step)
        return (z * 4 + moved if axis == 0 else moved * 4 + y, tp)

    def remote(src, dst, send, recv, device):
        return pltpu.make_async_remote_copy(
            src_ref=src, dst_ref=dst, send_sem=send, recv_sem=recv,
            device_id=device, device_id_type=pl.DeviceIdType.MESH,
        )

    barrier = pltpu.get_barrier_semaphore()
    for axis in (0, 1):
        for step in (1, -1):
            pl.semaphore_signal(
                barrier, inc=1, device_id=peer(axis, step), device_id_type=pl.DeviceIdType.MESH
            )
    lat_copy = pltpu.make_async_copy(lat_hbm, lat, lat_sem)
    lat_copy.start()

    qpos = (y, z)
    kpos = (z, y)
    wide[0] = q_ref[...].astype(F32)
    wide[1] = k_ref[...].astype(F32)
    wide[2] = v_ref[...].astype(F32)
    wide[3] = og_ref[...].astype(F32)
    for h in (0, 1):
        qdo[h, qpos[h], 0] = wide[0, pl.ds(h, T, stride=2), :].astype(BF16)
        kv[h, kpos[h], 0] = wide[1, pl.ds(h, T, stride=2), :].astype(BF16)
        kv[h, kpos[h], 1] = wide[2, pl.ds(h, T, stride=2), :].astype(BF16)
    pl.semaphore_wait(barrier, 4)

    qh = (0, 1)
    kh = (1, 0)
    first = {}

    def item(axis, name, slot):
        if name == "q":
            return qdo.at[qh[axis], slot, 0]
        if name == "do":
            return qdo.at[qh[axis], slot, 1]
        if name == "st":
            return st.at[qh[axis], slot]
        if name == "k":
            return kv.at[kh[axis], slot, 0]
        return kv.at[kh[axis], slot, 1]

    names = ("q", "k", "v", "do", "st")

    def send_own(some):
        for name in some:
            for axis in (0, 1):
                for d, step in enumerate((1, -1)):
                    n = names.index(name)
                    ref = item(axis, name, pos[axis])
                    c = remote(ref, ref, gs.at[axis, d, n], gr.at[axis, d, n], peer(axis, step))
                    c.start()
                    first[axis, d, name] = c

    send_own(("q", "k", "v"))

    wide2[...] = mo_ref[...].astype(F32)
    gain = gain_ref[...]
    for h in (0, 1):
        lam = lam_ref[h]
        m1 = wide2[pl.ds(h, T, stride=4), :]
        m2 = wide2[pl.ds(2 + h, T, stride=4), :]
        comb = m1 - lam * m2
        inv = lax.rsqrt(jnp.mean(comb * comb, axis=-1, keepdims=True) + EPSILON)
        wtd = gain * wide[3, pl.ds(h, T, stride=2), :]
        cross = jnp.mean(comb * wtd, axis=-1, keepdims=True)
        grad = (inv * wtd - inv * inv * inv * comb * cross).astype(BF16)
        qdo[h, qpos[h], 1] = grad
        gf = grad.astype(F32)
        r1 = jnp.sum(jnp.transpose(gf * m1), axis=0, keepdims=True)
        r2 = jnp.sum(jnp.transpose(gf * m2), axis=0, keepdims=True)
        lam_row = jnp.full((1, T), lam, F32)
        st[h, qpos[h], 0:1] = lse_ref[2 * h : 2 * h + 1, :] * LOG2E
        st[h, qpos[h], 1:2] = (lse_ref[2 * h + 1 : 2 * h + 2, :] - jnp.log(lam_row)) * LOG2E
        st[h, qpos[h], 2:3] = r1
        st[h, qpos[h], 3:4] = r2
        st[h, qpos[h], 4:8] = jnp.zeros((4, T), F32)
    send_own(("do", "st"))

    dqt[...] = jnp.zeros_like(dqt)
    dkv[...] = jnp.zeros_like(dkv)

    lane = lax.broadcasted_iota(jnp.int32, (T, W), 1)

    def unit(h, qs, ks, masked):
        q = qdo[h, qs, 0]
        do = qdo[h, qs, 1]
        k = kv[h, ks, 0]
        v = kv[h, ks, 1]
        zero = jnp.zeros_like(q)
        q1 = jnp.where(lane < 64, q, zero)
        q2 = jnp.where(lane < 64, zero, -q)
        s1 = dot_nt(k, q1)
        s2 = dot_nt(k, q2)
        dp = dot_nt(v, do)
        p1 = jnp.exp2(s1 * (SCALE * LOG2E) - st[h, qs, 0:1])
        p2 = jnp.exp2(s2 * (-SCALE * LOG2E) - st[h, qs, 1:2])
        if masked:
            rows = lax.broadcasted_iota(jnp.int32, (T, T), 0)
            cols = lax.broadcasted_iota(jnp.int32, (T, T), 1)
            keep = rows <= cols
            p1 = jnp.where(keep, p1, 0.0)
            p2 = jnp.where(keep, p2, 0.0)
        w = (p1 - p2).astype(BF16)
        d1 = (p1 * (dp - st[h, qs, 2:3])).astype(BF16)
        d2 = (p2 * (dp - st[h, qs, 3:4])).astype(BF16)
        kt = jnp.transpose(k)
        dqt[h, qs, 0:64] += dot(kt[0:64], d1)
        dqt[h, qs, 64:128] -= dot(kt[64:128], d2)
        dkv[h, ks, 0] += dot(d1, q1) + dot(d2, q2)
        dkv[h, ks, 1] += dot(w, do)

    unit(0, y, z, True)
    unit(1, z, y, True)

    second = []
    for axis in (0, 1):
        for d, some in ((0, ("q", "k")), (1, ("do", "v", "st"))):
            for name in some:
                first[axis, d, name].wait_recv()
                step = 1 if d == 0 else -1
                ref = item(axis, name, ring(axis, -step))
                n = 5 + names.index(name)
                c = remote(ref, ref, gs.at[axis, d, n], gr.at[axis, d, n], peer(axis, step))
                c.start()
                second.append(c)
    for axis in (0, 1):
        for d, some in ((1, ("q", "k")), (0, ("do", "v", "st"))):
            for name in some:
                first[axis, d, name].wait_recv()
    for c in second:
        c.wait_recv()

    count_a = 4 * z + 3 - y

    def step_unit(n, carry):
        i = n + jnp.where(n >= 4 * z, y + 1, 0)
        u = n - count_a
        w = u - y
        in_a = n < count_a
        h = jnp.where(in_a, 0, 1)
        near = u < y
        qs = jnp.where(in_a, i % 4, jnp.where(near, z, z + 1 + w // 4))
        ks = jnp.where(in_a, i // 4, jnp.where(near, u, (w + 4) % 4))
        unit(h, qs, ks, False)
        return carry

    lax.fori_loop(0, 15, step_unit, 0)

    def reduce_start(tx, rx, axis, base, get):
        out = []

        def go(j, value, step):
            tx[axis, j] = value.astype(BF16)
            c = remote(
                tx.at[axis, j], rx.at[axis, j], rs.at[axis, base + j], rr.at[axis, base + j],
                peer(axis, step),
            )
            c.start()
            out.append(c)

        far, up, down = ring(axis, 2), ring(axis, 1), ring(axis, -1)
        go(0, get(far, 0), 1)
        go(1, get(far, 1), -1)
        go(2, get(up, 1), 1)
        go(3, get(down, 0), -1)
        return (out, go)

    def reduce_middle(state, tx, rx, axis, get):
        out, go = state
        up, down = ring(axis, 1), ring(axis, -1)
        mine = get(up, 0)
        out[0].wait_recv()
        go(4, mine + rx[axis, 0].astype(F32), 1)
        mine = get(down, 1)
        out[1].wait_recv()
        go(5, mine + rx[axis, 1].astype(F32), -1)

    def reduce_end(state, rx, axis, get):
        out, _ = state
        own0 = get(pos[axis], 0)
        own1 = get(pos[axis], 1)
        for j in (2, 3, 4, 5):
            out[j].wait_recv()
        r0 = own0 + rx[axis, 3].astype(F32) + rx[axis, 4].astype(F32)
        r1 = own1 + rx[axis, 2].astype(F32) + rx[axis, 5].astype(F32)
        return r0, r1

    def get_dq(h):
        return lambda slot, p: dqt[h, slot, 64 * p : 64 * p + 64] * SCALE

    def get_dkv(h):
        return lambda slot, p: dkv[h, slot, p] * (SCALE if p == 0 else 1.0)

    dq_state = {}
    for h in (0, 1):
        dq_state[h] = reduce_start(qtx, qrx, h, 0, get_dq(h))
    for h in (0, 1):
        reduce_middle(dq_state[h], qtx, qrx, h, get_dq(h))
    lat_copy.wait()

    def block_a(z_to, y_to):
        return z_to * 4 + y_to

    def get_wg(h):
        def get(slot, p):
            parts = []
            for o in (2 * p, 2 * p + 1):
                blk = block_a(o, slot) if h == 0 else block_a(slot, o)
                cols = lat[:, pl.ds(pl.multiple_of(blk * T, T), T)]
                parts.append(dot(dqf[h], cols))
            return jnp.stack(parts)

        return get

    a_state = {}
    for h in (0, 1):
        r0, r1 = reduce_end(dq_state[h], qrx, h, get_dq(h))
        dqf[h, 0:64] = r0.astype(BF16)
        dqf[h, 64:128] = r1.astype(BF16)
        a_state[h] = reduce_start(atx, arx, h, 6, get_wg(h))

    k_state = {}
    for axis in (0, 1):
        k_state[axis] = reduce_start(ktx, krx, axis, 18, get_dkv(1 - axis))
    for h in (0, 1):
        wide[0, pl.ds(h, T, stride=2), :] = jnp.transpose(dqf[h].astype(F32))
    qg_ref[...] = wide[0].astype(BF16)
    for h in (0, 1):
        reduce_middle(a_state[h], atx, arx, h, get_wg(h))
    for axis in (0, 1):
        reduce_middle(k_state[axis], ktx, krx, axis, get_dkv(1 - axis))
    b_state = {}
    b_get = {}
    for h in (0, 1):
        r0, r1 = reduce_end(a_state[h], arx, h, get_wg(h))
        wide_b = wide2
        for o in range(4):
            part = r0[o] if o < 2 else r1[o - 2]
            wide_b[pl.ds(o * 128, 128), :] = part[:, 0:128] if h == 0 else part[:, 0:128]
            wide_b[pl.ds(512 + o * 128, 128), :] = part[:, 128:256]

        def get(slot, p):
            start = pl.multiple_of(slot * 128 + 64 * p, 64)
            return jnp.concatenate(
                [wide2[pl.ds(start, 64), :], wide2[pl.ds(start + 512, 64), :]], axis=1
            )

        other = 1 - h
        own = (get(pos[other], 0), get(pos[other], 1))
        ups = (get(ring(other, 1), 0), get(ring(other, -1), 1))
        b_state[h] = reduce_start(btx, brx, other, 12, get)
        b_get[h] = (own, ups)
    for h in (0, 1):
        own, ups = b_get[h]
        other = 1 - h
        out, go = b_state[h]
        out[0].wait_recv()
        go(4, ups[0] + brx[other, 0].astype(F32), 1)
        out[1].wait_recv()
        go(5, ups[1] + brx[other, 1].astype(F32), -1)
    for axis in (0, 1):
        h = 1 - axis
        r0, r1 = reduce_end(k_state[axis], krx, axis, get_dkv(h))
        wide[1, pl.ds(h, T, stride=2), :] = r0
        wide[2, pl.ds(h, T, stride=2), :] = r1
    kg_ref[...] = wide[1].astype(BF16)
    vg_ref[...] = wide[2].astype(BF16)
    for h in (0, 1):
        own, _ = b_get[h]
        other = 1 - h
        r0, r1 = reduce_end(b_state[h], brx, other, lambda slot, p: own[p])
        wg_ref[:, h * W : h * W + W] = jnp.transpose(jnp.concatenate([r0, r1], axis=0))

    for c in first.values():
        c.wait_send()
    for c in second:
        c.wait_send()
    for states in (dq_state, a_state, k_state, b_state):
        for out, _ in states.values():
            for c in out:
                c.wait_send()


def body(latents, query_heads, key_heads, value_heads, map_outputs, log_sums, out_grad, mix_lambda, norm_gain):
    rows = 2 * T
    vmem = pl.BlockSpec(memory_space=pltpu.VMEM)
    outs = pl.pallas_call(
        kernel,
        out_shape=(
            jax.ShapeDtypeStruct((rows, W), BF16),
            jax.ShapeDtypeStruct((rows, W), BF16),
            jax.ShapeDtypeStruct((rows, W), BF16),
            jax.ShapeDtypeStruct((T, 2 * W), F32),
        ),
        in_specs=[
            vmem, vmem, vmem, vmem, vmem, vmem,
            pl.BlockSpec(memory_space=pltpu.SMEM), vmem,
            pl.BlockSpec(memory_space=pl.ANY),
        ],
        out_specs=(vmem, vmem, vmem, vmem),
        scratch_shapes=[
            pltpu.VMEM((T, 4096), BF16),
            pltpu.VMEM((2, 4, 2, T, W), BF16),
            pltpu.VMEM((2, 4, 2, T, W), BF16),
            pltpu.VMEM((2, 4, 8, T), F32),
            pltpu.VMEM((2, 4, W, T), F32),
            pltpu.VMEM((2, 4, 2, T, W), F32),
            pltpu.VMEM((4, rows, W), F32),
            pltpu.VMEM((4 * T, W), F32),
            pltpu.VMEM((2, W, T), BF16),
            pltpu.VMEM((2, 6, 64, T), BF16),
            pltpu.VMEM((2, 6, 64, T), BF16),
            pltpu.VMEM((2, 6, T, W), BF16),
            pltpu.VMEM((2, 6, T, W), BF16),
            pltpu.VMEM((2, 6, 2, W, T), BF16),
            pltpu.VMEM((2, 6, 2, W, T), BF16),
            pltpu.VMEM((2, 6, 64, T), BF16),
            pltpu.VMEM((2, 6, 64, T), BF16),
            pltpu.SemaphoreType.DMA,
            pltpu.SemaphoreType.DMA((2, 2, 10)),
            pltpu.SemaphoreType.DMA((2, 2, 10)),
            pltpu.SemaphoreType.DMA((2, 24)),
            pltpu.SemaphoreType.DMA((2, 24)),
        ],
        compiler_params=pltpu.CompilerParams(
            collective_id=0, has_side_effects=True, vmem_limit_bytes=48 * 1024 * 1024
        ),
    )(
        query_heads.reshape(rows, W),
        key_heads.reshape(rows, W),
        value_heads.reshape(rows, W),
        map_outputs.reshape(2 * rows, W),
        jnp.transpose(log_sums, (1, 2, 0)).reshape(4, T),
        out_grad.reshape(rows, W),
        mix_lambda,
        norm_gain.reshape(1, W),
        latents,
    )
    qg, kg, vg, wg = outs
    shape = query_heads.shape
    return (qg.reshape(shape), kg.reshape(shape), vg.reshape(shape), wg)


def solution(mesh):
    placed = (
        P("sp", None),
        P("sp", "tp", None),
        P("sp", "tp", None),
        P("sp", "tp", None),
        P("sp", None, "tp", None),
        P("sp", "tp", None),
        P("sp", "tp", None),
        P("tp"),
        P(),
    )
    return jax.shard_map(
        body,
        mesh=mesh,
        in_specs=placed,
        out_specs=(P("sp", "tp", None), P("sp", "tp", None), P("sp", "tp", None), P("sp", "tp")),
        check_vma=False,
    )
```

```python
import functools

import jax
import jax.numpy as jnp
from jax import lax
from jax.experimental import pallas as pl
from jax.experimental.pallas import tpu as pltpu
from jax.sharding import PartitionSpec as P

F32 = jnp.float32
BF16 = jnp.bfloat16
EPSILON = 1e-05
LOG2E = 1.4426950408889634
SCALE = 0.125
T = 256
W = 128
VMEM_ALL = 67043328
NT = (((1,), (1,)), ((), ()))


def dot(a, b):
    return jnp.dot(a, b, preferred_element_type=F32)


def dot_nt(a, b):
    return lax.dot_general(a, b, NT, preferred_element_type=F32)


def kernel(
    q_hbm, k_hbm, v_hbm, mo_hbm, lse_hbm, og_hbm, lam_hbm, gain_hbm, lat_hbm,
    qg_hbm, kg_hbm, vg_hbm, wg_hbm,
    q_in, k_in, v_in, mo_in, lse_in, og_in, lam_in, gain_in,
    lat, qdo, kv, st, dqt, dkv, wide, wide2, dqf,
    qtx, qrx, ktx, krx, atx, arx, btx, brx,
    qg_ref, kg_ref, vg_ref, wg_ref,
    in_sem, out_sem, gs, gr, rs, rr,
):
    sp = lax.axis_index("sp")
    tp = lax.axis_index("tp")
    z = sp // 4
    y = sp % 4
    pos = (y, z)

    def ring(axis, step):
        return lax.rem(pos[axis] + step + 4, 4)

    def peer(axis, step):
        moved = ring(axis, step)
        return (z * 4 + moved if axis == 0 else moved * 4 + y, tp)

    def remote(src, dst, send, recv, device):
        return pltpu.make_async_remote_copy(
            src_ref=src, dst_ref=dst, send_sem=send, recv_sem=recv,
            device_id=device, device_id_type=pl.DeviceIdType.MESH,
        )

    barrier = pltpu.get_barrier_semaphore()
    for axis in (0, 1):
        for step in (1, -1):
            pl.semaphore_signal(
                barrier, inc=1, device_id=peer(axis, step), device_id_type=pl.DeviceIdType.MESH
            )
    sources = (q_hbm, k_hbm, v_hbm, og_hbm, mo_hbm, lse_hbm, lam_hbm, gain_hbm, lat_hbm)
    targets = (q_in, k_in, v_in, og_in, mo_in, lse_in, lam_in, gain_in, lat)
    loads = [pltpu.make_async_copy(a, b, in_sem.at[n]) for n, (a, b) in enumerate(zip(sources, targets))]
    for c in loads:
        c.start()

    qpos = (y, z)
    kpos = (z, y)
    for n, ref in enumerate((q_in, k_in, v_in)):
        loads[n].wait()
        wide[n] = ref[...].astype(F32)
    for h in (0, 1):
        qdo[h, qpos[h], 0] = wide[0, pl.ds(h, T, stride=2), :].astype(BF16)
        kv[h, kpos[h], 0] = wide[1, pl.ds(h, T, stride=2), :].astype(BF16)
        kv[h, kpos[h], 1] = wide[2, pl.ds(h, T, stride=2), :].astype(BF16)
    pl.semaphore_wait(barrier, 4)

    qh = (0, 1)
    kh = (1, 0)
    first = {}

    def item(axis, name, slot):
        if name == "q":
            return qdo.at[qh[axis], slot, 0]
        if name == "do":
            return qdo.at[qh[axis], slot, 1]
        if name == "st":
            return st.at[qh[axis], slot]
        if name == "k":
            return kv.at[kh[axis], slot, 0]
        return kv.at[kh[axis], slot, 1]

    names = ("q", "k", "v", "do", "st")

    def send_own(some):
        for name in some:
            for axis in (0, 1):
                for d, step in enumerate((1, -1)):
                    n = names.index(name)
                    ref = item(axis, name, pos[axis])
                    c = remote(ref, ref, gs.at[axis, d, n], gr.at[axis, d, n], peer(axis, step))
                    c.start()
                    first[axis, d, name] = c

    send_own(("q", "k", "v"))

    for c in loads[3:8]:
        c.wait()
    wide[3] = og_in[...].astype(F32)
    wide2[...] = mo_in[...].astype(F32)
    gain = gain_in[...]
    for h in (0, 1):
        lam = lam_in[h]
        m1 = wide2[pl.ds(h, T, stride=4), :]
        m2 = wide2[pl.ds(2 + h, T, stride=4), :]
        comb = m1 - lam * m2
        inv = lax.rsqrt(jnp.mean(comb * comb, axis=-1, keepdims=True) + EPSILON)
        wtd = gain * wide[3, pl.ds(h, T, stride=2), :]
        cross = jnp.mean(comb * wtd, axis=-1, keepdims=True)
        grad = (inv * wtd - inv * inv * inv * comb * cross).astype(BF16)
        qdo[h, qpos[h], 1] = grad
        gf = grad.astype(F32)
        r1 = jnp.sum(jnp.transpose(gf * m1), axis=0, keepdims=True)
        r2 = jnp.sum(jnp.transpose(gf * m2), axis=0, keepdims=True)
        lam_row = jnp.full((1, T), lam, F32)
        st[h, qpos[h], 0:1] = lse_in[h, 0:1, :] * LOG2E
        st[h, qpos[h], 1:2] = (lse_in[h, 1:2, :] - jnp.log(lam_row)) * LOG2E
        st[h, qpos[h], 2:3] = r1
        st[h, qpos[h], 3:4] = r2
        st[h, qpos[h], 4:8] = jnp.zeros((4, T), F32)
    send_own(("do", "st"))

    dqt[...] = jnp.zeros_like(dqt)
    dkv[...] = jnp.zeros_like(dkv)

    lane = lax.broadcasted_iota(jnp.int32, (T, W), 1)

    def unit(h, qs, ks, masked):
        q = qdo[h, qs, 0]
        do = qdo[h, qs, 1]
        k = kv[h, ks, 0]
        v = kv[h, ks, 1]
        zero = jnp.zeros_like(q)
        q1 = jnp.where(lane < 64, q, zero)
        q2 = jnp.where(lane < 64, zero, -q)
        s1 = dot_nt(k, q1)
        s2 = dot_nt(k, q2)
        dp = dot_nt(v, do)
        p1 = jnp.exp2(s1 * (SCALE * LOG2E) - st[h, qs, 0:1])
        p2 = jnp.exp2(s2 * (-SCALE * LOG2E) - st[h, qs, 1:2])
        if masked:
            rows = lax.broadcasted_iota(jnp.int32, (T, T), 0)
            cols = lax.broadcasted_iota(jnp.int32, (T, T), 1)
            keep = rows <= cols
            p1 = jnp.where(keep, p1, 0.0)
            p2 = jnp.where(keep, p2, 0.0)
        w = (p1 - p2).astype(BF16)
        d1 = (p1 * (dp - st[h, qs, 2:3])).astype(BF16)
        d2 = (p2 * (dp - st[h, qs, 3:4])).astype(BF16)
        kt = jnp.transpose(k)
        dqt[h, qs, 0:64] += dot(kt[0:64], d1)
        dqt[h, qs, 64:128] -= dot(kt[64:128], d2)
        dkv[h, ks, 0] += dot(d1, q1) + dot(d2, q2)
        dkv[h, ks, 1] += dot(w, do)

    def maybe_unit(h, i, j):
        qo = jnp.where(i < 2, i, 5 - i)
        ko = jnp.where(j < 2, j, 5 - j)
        qbase = jnp.where(h == 0, y, z)
        kbase = jnp.where(h == 0, z, y)
        qs = (qbase + qo) % 4
        ks = (kbase + ko) % 4
        q_block = jnp.where(h == 0, z * 4 + qs, qs * 4 + y)
        k_block = jnp.where(h == 0, ks * 4 + y, z * 4 + ks)

        @pl.when(k_block < q_block)
        def _():
            unit(h, qs, ks, False)

    unit(0, y, z, True)
    unit(1, z, y, True)

    second = []
    for some in (("q", "k"), ("v",), ("do", "st")):
        for axis in (0, 1):
            for name in some:
                for d in (0, 1):
                    first[axis, d, name].wait_recv()
                    if d == (0 if name in ("q", "k") else 1):
                        step = 1 if d == 0 else -1
                        ref = item(axis, name, ring(axis, -step))
                        n = 5 + names.index(name)
                        c = remote(ref, ref, gs.at[axis, d, n], gr.at[axis, d, n], peer(axis, step))
                        c.start()
                        second.append(c)

    def near_units(n, carry):
        h = n // 8
        m = n % 8 + 1
        maybe_unit(h, m // 3, m % 3)
        return carry

    lax.fori_loop(0, 16, near_units, 0)
    for c in second:
        c.wait_recv()

    def far_queries(n, carry):
        maybe_unit(n // 4, jnp.int32(3), n % 4)
        return carry

    def far_keys(n, carry):
        maybe_unit(n // 3, n % 3, jnp.int32(3))
        return carry

    class Reduction:
        def __init__(self, tx, rx, axis, base, get):
            self.tx, self.rx, self.axis, self.base, self.get = tx, rx, axis, base, get
            self.out = {}

        def go(self, j, value, step):
            axis = self.axis
            self.tx[axis, j] = value.astype(BF16)
            c = remote(
                self.tx.at[axis, j], self.rx.at[axis, j],
                rs.at[axis, self.base + j], rr.at[axis, self.base + j], peer(axis, step),
            )
            c.start()
            self.out[j] = c

        def far(self):
            slot = ring(self.axis, 2)
            self.go(0, self.get(slot, 0), 1)
            self.go(1, self.get(slot, 1), -1)

        def direct(self):
            self.go(2, self.get(ring(self.axis, 1), 1), 1)
            self.go(3, self.get(ring(self.axis, -1), 0), -1)

        def summed(self):
            for j, step in ((0, 1), (1, -1)):
                mine = self.get(ring(self.axis, step), j)
                self.out[j].wait_recv()
                self.go(4 + j, mine + self.rx[self.axis, j].astype(F32), step)

        def end(self):
            own0 = self.get(pos[self.axis], 0)
            own1 = self.get(pos[self.axis], 1)
            for j in (2, 3, 4, 5):
                self.out[j].wait_recv()
            rx = self.rx
            r0 = own0 + rx[self.axis, 3].astype(F32) + rx[self.axis, 4].astype(F32)
            r1 = own1 + rx[self.axis, 2].astype(F32) + rx[self.axis, 5].astype(F32)
            return r0, r1

        def drain(self):
            for c in self.out.values():
                c.wait_send()

    def get_dq(h):
        return lambda slot, p: dqt[h, slot, 64 * p : 64 * p + 64] * SCALE

    def get_dkv(h):
        return lambda slot, p: dkv[h, slot, p] * (SCALE if p == 0 else 1.0)

    def get_wg(h):
        def get(slot, p):
            parts = []
            for o in (2 * p, 2 * p + 1):
                blk = o * 4 + slot if h == 0 else slot * 4 + o
                cols = lat[:, pl.ds(pl.multiple_of(blk * T, T), T)]
                parts.append(dot(dqf[h], cols))
            return jnp.stack(parts)

        return get

    def get_last(h):
        def get(slot, p):
            start = pl.multiple_of(slot * 128 + 64 * p, 64)
            return jnp.concatenate(
                [wide[h, pl.ds(start, 64), :], wide[2 + h, pl.ds(start, 64), :]], axis=1
            )

        return get

    both = (0, 1)
    dq = [Reduction(qtx, qrx, h, 0, get_dq(h)) for h in both]
    dk = [Reduction(ktx, krx, 1 - h, 18, get_dkv(h)) for h in both]
    wa = [Reduction(atx, arx, h, 6, get_wg(h)) for h in both]
    wb = [Reduction(btx, brx, 1 - h, 12, get_last(h)) for h in both]

    lax.fori_loop(0, 8, far_queries, 0)
    for h in both:
        dq[h].far()
    lax.fori_loop(0, 6, far_keys, 0)
    for h in both:
        dq[h].direct()
    for h in both:
        dq[h].summed()
    for h in both:
        dk[h].far()
    for h in both:
        dk[h].direct()
    for h in both:
        dk[h].summed()
    loads[8].wait()
    for h in both:
        r0, r1 = dq[h].end()
        dqf[h, 0:64] = r0.astype(BF16)
        dqf[h, 64:128] = r1.astype(BF16)
        wa[h].far()
    for h in both:
        wa[h].direct()
    for h in both:
        wa[h].summed()
    for h in both:
        wide2[pl.ds(h, T, stride=2), :] = jnp.transpose(dqf[h].astype(F32))
    qg_ref[...] = wide2[0 : 2 * T, :].astype(BF16)
    stores = [
        pltpu.make_async_copy(a, b, out_sem.at[n])
        for n, (a, b) in enumerate(
            ((qg_ref, qg_hbm), (kg_ref, kg_hbm), (vg_ref, vg_hbm), (wg_ref, wg_hbm))
        )
    ]
    stores[0].start()
    for h in both:
        r0, r1 = wa[h].end()
        for o in range(4):
            part = r0[o] if o < 2 else r1[o - 2]
            wide[h, pl.ds(o * 128, 128), :] = part[:, 0:128]
            wide[2 + h, pl.ds(o * 128, 128), :] = part[:, 128:256]
        wb[h].far()
        wb[h].direct()
    for h in both:
        wb[h].summed()
    for p, ref in ((0, kg_ref), (1, vg_ref)):
        for h in both:
            if p == 0:
                ends = dk[h].end()
                dk[h].ends = ends
            wide2[pl.ds(2 * T * p + h, T, stride=2), :] = dk[h].ends[p]
        ref[...] = wide2[2 * T * p : 2 * T * p + 2 * T, :].astype(BF16)
        stores[1 + p].start()
    for h in both:
        r0, r1 = wb[h].end()
        wg_ref[:, h * W : h * W + W] = jnp.transpose(jnp.concatenate([r0, r1], axis=0))
    stores[3].start()

    for c in first.values():
        c.wait_send()
    for c in second:
        c.wait_send()
    for group in (dq, dk, wa, wb):
        for r in group:
            r.drain()
    for c in stores:
        c.wait()


def put_kernel(*refs):
    sources, targets, rooms, sems = refs[0:4], refs[4:8], refs[8:12], refs[12]
    reads = [pltpu.make_async_copy(sources[n], rooms[n], sems.at[n]) for n in range(4)]
    writes = [pltpu.make_async_copy(rooms[n], targets[n], sems.at[4 + n]) for n in range(4)]
    for c in reads:
        c.start()
    for n in range(4):
        reads[n].wait()
        writes[n].start()
    for c in writes:
        c.wait()


def body(latents, query_heads, key_heads, value_heads, map_outputs, log_sums, out_grad, mix_lambda, norm_gain):
    rows = 2 * T
    hbm = pl.BlockSpec(memory_space=pltpu.HBM)
    out_shape = (
        jax.ShapeDtypeStruct((rows, W), BF16),
        jax.ShapeDtypeStruct((rows, W), BF16),
        jax.ShapeDtypeStruct((rows, W), BF16),
        jax.ShapeDtypeStruct((T, 2 * W), F32),
    )
    outs = pl.pallas_call(
        kernel,
        out_shape=out_shape,
        in_specs=[hbm] * 9,
        out_specs=(hbm, hbm, hbm, hbm),
        scratch_shapes=[
            pltpu.VMEM((rows, W), BF16),
            pltpu.VMEM((rows, W), BF16),
            pltpu.VMEM((rows, W), BF16),
            pltpu.VMEM((2 * rows, W), BF16),
            pltpu.VMEM((2, 2, T), F32),
            pltpu.VMEM((rows, W), BF16),
            pltpu.SMEM((2,), F32),
            pltpu.VMEM((1, W), F32),
            pltpu.VMEM((T, 4096), BF16),
            pltpu.VMEM((2, 4, 2, T, W), BF16),
            pltpu.VMEM((2, 4, 2, T, W), BF16),
            pltpu.VMEM((2, 4, 8, T), F32),
            pltpu.VMEM((2, 4, W, T), F32),
            pltpu.VMEM((2, 4, 2, T, W), F32),
            pltpu.VMEM((4, rows, W), F32),
            pltpu.VMEM((4 * T, W), F32),
            pltpu.VMEM((2, W, T), BF16),
            pltpu.VMEM((2, 6, 64, T), BF16),
            pltpu.VMEM((2, 6, 64, T), BF16),
            pltpu.VMEM((2, 6, T, W), BF16),
            pltpu.VMEM((2, 6, T, W), BF16),
            pltpu.VMEM((2, 6, 2, W, T), BF16),
            pltpu.VMEM((2, 6, 2, W, T), BF16),
            pltpu.VMEM((2, 6, 64, T), BF16),
            pltpu.VMEM((2, 6, 64, T), BF16),
            pltpu.VMEM((rows, W), BF16),
            pltpu.VMEM((rows, W), BF16),
            pltpu.VMEM((rows, W), BF16),
            pltpu.VMEM((T, 2 * W), F32),
            pltpu.SemaphoreType.DMA((9,)),
            pltpu.SemaphoreType.DMA((4,)),
            pltpu.SemaphoreType.DMA((2, 2, 10)),
            pltpu.SemaphoreType.DMA((2, 2, 10)),
            pltpu.SemaphoreType.DMA((2, 24)),
            pltpu.SemaphoreType.DMA((2, 24)),
        ],
        compiler_params=pltpu.CompilerParams(
            collective_id=0, has_side_effects=True, vmem_limit_bytes=VMEM_ALL
        ),
    )(
        query_heads.reshape(rows, W),
        key_heads.reshape(rows, W),
        value_heads.reshape(rows, W),
        map_outputs.reshape(2 * rows, W),
        jnp.transpose(log_sums, (1, 2, 0)),
        out_grad.reshape(rows, W),
        mix_lambda,
        norm_gain.reshape(1, W),
        latents,
    )
    qg, kg, vg, wg = pl.pallas_call(
        put_kernel,
        out_shape=out_shape,
        in_specs=[hbm] * 4,
        out_specs=(hbm, hbm, hbm, hbm),
        scratch_shapes=[pltpu.VMEM(o.shape, o.dtype) for o in out_shape]
        + [pltpu.SemaphoreType.DMA((8,))],
        compiler_params=pltpu.CompilerParams(vmem_limit_bytes=VMEM_ALL),
    )(*outs)
    shape = query_heads.shape
    return (qg.reshape(shape), kg.reshape(shape), vg.reshape(shape), wg)


def solution(mesh):
    placed = (
        P("sp", None),
        P("sp", "tp", None),
        P("sp", "tp", None),
        P("sp", "tp", None),
        P("sp", None, "tp", None),
        P("sp", "tp", None),
        P("sp", "tp", None),
        P("tp"),
        P(),
    )
    return jax.shard_map(
        body,
        mesh=mesh,
        in_specs=placed,
        out_specs=(P("sp", "tp", None), P("sp", "tp", None), P("sp", "tp", None), P("sp", "tp")),
        check_vma=False,
    )
```

```python
import functools

import jax
import jax.numpy as jnp
from jax import lax
from jax.experimental import pallas as pl
from jax.experimental.pallas import tpu as pltpu
from jax.sharding import PartitionSpec as P

F32 = jnp.float32
BF16 = jnp.bfloat16
EPSILON = 1e-05
LOG2E = 1.4426950408889634
SCALE = 0.125
T = 256
W = 128
VMEM_ALL = 66200000
NT = (((1,), (1,)), ((), ()))


def dot(a, b):
    return jnp.dot(a, b, preferred_element_type=F32)


def dot_nt(a, b):
    return lax.dot_general(a, b, NT, preferred_element_type=F32)


def kernel(
    q_hbm, k_hbm, v_hbm, mo_hbm, lse_hbm, og_hbm, lam_hbm, gain_hbm, lat_hbm,
    qg_ref, kg_ref, vg_ref, wg_ref,
    q_in, k_in, v_in, mo_in, lse_in, og_in, lam_in, gain_in,
    lat, qdo, kv, st, dqt, dkv, wds, wide, wide2, dqf,
    qtx, qrx, ktx, krx, atx, arx, btx, brx,
    in_sem, gs, gr, rs, rr,
):
    sp = lax.axis_index("sp")
    tp = lax.axis_index("tp")
    z = sp // 4
    y = sp % 4
    pos = (y, z)

    def ring(axis, step):
        return lax.rem(pos[axis] + step + 4, 4)

    def peer(axis, step):
        moved = ring(axis, step)
        return (z * 4 + moved if axis == 0 else moved * 4 + y, tp)

    def remote(src, dst, send, recv, device):
        return pltpu.make_async_remote_copy(
            src_ref=src, dst_ref=dst, send_sem=send, recv_sem=recv,
            device_id=device, device_id_type=pl.DeviceIdType.MESH,
        )

    barrier = pltpu.get_barrier_semaphore()
    for axis in (0, 1):
        for step in (1, -1):
            pl.semaphore_signal(
                barrier, inc=1, device_id=peer(axis, step), device_id_type=pl.DeviceIdType.MESH
            )
    sources = (q_hbm, k_hbm, v_hbm, og_hbm, mo_hbm, lse_hbm, lam_hbm, gain_hbm, lat_hbm)
    targets = (q_in, k_in, v_in, og_in, mo_in, lse_in, lam_in, gain_in, lat)
    loads = [pltpu.make_async_copy(a, b, in_sem.at[n]) for n, (a, b) in enumerate(zip(sources, targets))]
    for c in loads:
        c.start()

    qpos = (y, z)
    kpos = (z, y)
    for n, ref in enumerate((q_in, k_in, v_in)):
        loads[n].wait()
        wide[n] = ref[...].astype(F32)
    for h in (0, 1):
        qdo[h, qpos[h], 0] = wide[0, pl.ds(h, T, stride=2), :].astype(BF16)
        kv[h, kpos[h], 0] = wide[1, pl.ds(h, T, stride=2), :].astype(BF16)
        kv[h, kpos[h], 1] = wide[2, pl.ds(h, T, stride=2), :].astype(BF16)
    pl.semaphore_wait(barrier, 4)

    qh = (0, 1)
    kh = (1, 0)
    first = {}

    def item(axis, name, slot):
        if name == "q":
            return qdo.at[qh[axis], slot, 0]
        if name == "do":
            return qdo.at[qh[axis], slot, 1]
        if name == "st":
            return st.at[qh[axis], slot]
        if name == "k":
            return kv.at[kh[axis], slot, 0]
        return kv.at[kh[axis], slot, 1]

    names = ("q", "k", "v", "do", "st")

    def send_own(some):
        for name in some:
            for axis in (0, 1):
                for d, step in enumerate((1, -1)):
                    n = names.index(name)
                    ref = item(axis, name, pos[axis])
                    c = remote(ref, ref, gs.at[axis, d, n], gr.at[axis, d, n], peer(axis, step))
                    c.start()
                    first[axis, d, name] = c

    send_own(("q", "k", "v"))

    for c in loads[3:8]:
        c.wait()
    wide[3] = og_in[...].astype(F32)
    wide2[...] = mo_in[...].astype(F32)
    gain = gain_in[...]
    for h in (0, 1):
        lam = lam_in[h]
        m1 = wide2[pl.ds(h, T, stride=4), :]
        m2 = wide2[pl.ds(2 + h, T, stride=4), :]
        comb = m1 - lam * m2
        inv = lax.rsqrt(jnp.mean(comb * comb, axis=-1, keepdims=True) + EPSILON)
        wtd = gain * wide[3, pl.ds(h, T, stride=2), :]
        cross = jnp.mean(comb * wtd, axis=-1, keepdims=True)
        grad = (inv * wtd - inv * inv * inv * comb * cross).astype(BF16)
        qdo[h, qpos[h], 1] = grad
        gf = grad.astype(F32)
        r1 = jnp.sum(jnp.transpose(gf * m1), axis=0, keepdims=True)
        r2 = jnp.sum(jnp.transpose(gf * m2), axis=0, keepdims=True)
        lam_row = jnp.full((1, T), lam, F32)
        st[h, qpos[h], 0:1] = lse_in[h, 0:1, :] * LOG2E
        st[h, qpos[h], 1:2] = (lse_in[h, 1:2, :] - jnp.log(lam_row)) * LOG2E
        st[h, qpos[h], 2:3] = r1
        st[h, qpos[h], 3:4] = r2
        st[h, qpos[h], 4:8] = jnp.zeros((4, T), F32)
    send_own(("do", "st"))

    dqt[...] = jnp.zeros_like(dqt)
    dkv[...] = jnp.zeros_like(dkv)

    lane = lax.broadcasted_iota(jnp.int32, (T, W), 1)

    def split_queries(h, qs):
        q = qdo[h, qs, 0]
        zero = jnp.zeros_like(q)
        return jnp.where(lane < 64, q, zero), jnp.where(lane < 64, zero, -q)

    def scores(h, qs, ks, masked):
        q1, q2 = split_queries(h, qs)
        do = qdo[h, qs, 1]
        half = T // 2
        for c in (0, half):
            k = kv[h, ks, 0, c : c + half]
            v = kv[h, ks, 1, c : c + half]
            s1 = dot_nt(k, q1)
            s2 = dot_nt(k, q2)
            dp = dot_nt(v, do)
            p1 = jnp.exp2(s1 * (SCALE * LOG2E) - st[h, qs, 0:1])
            p2 = jnp.exp2(s2 * (-SCALE * LOG2E) - st[h, qs, 1:2])
            if masked:
                rows = lax.broadcasted_iota(jnp.int32, (half, T), 0) + c
                cols = lax.broadcasted_iota(jnp.int32, (half, T), 1)
                keep = rows <= cols
                p1 = jnp.where(keep, p1, 0.0)
                p2 = jnp.where(keep, p2, 0.0)
            wds[0, c : c + half] = (p1 - p2).astype(BF16)
            wds[1, c : c + half] = (p1 * (dp - st[h, qs, 2:3])).astype(BF16)
            wds[2, c : c + half] = (p2 * (dp - st[h, qs, 3:4])).astype(BF16)

    def products(h, qs, ks):
        q1, q2 = split_queries(h, qs)
        w, d1, d2 = wds[0], wds[1], wds[2]
        kt = jnp.transpose(kv[h, ks, 0])
        dqt[h, qs, 0:64] += dot(kt[0:64], d1)
        dqt[h, qs, 64:128] -= dot(kt[64:128], d2)
        dkv[h, ks, 0] += dot(d1, q1) + dot(d2, q2)
        dkv[h, ks, 1] += dot(w, qdo[h, qs, 1])

    def maybe_unit(h, i, j, before):
        qo = jnp.where(i < 2, i, 5 - i)
        ko = jnp.where(j < 2, j, 5 - j)
        qbase = jnp.where(h == 0, y, z)
        kbase = jnp.where(h == 0, z, y)
        qs = (qbase + qo) % 4
        ks = (kbase + ko) % 4
        q_block = jnp.where(h == 0, z * 4 + qs, qs * 4 + y)
        k_block = jnp.where(h == 0, ks * 4 + y, z * 4 + ks)
        wanted = k_block < q_block

        @pl.when(wanted)
        def _():
            products(*before)
            scores(h, qs, ks, False)

        return tuple(jnp.where(wanted, a, b) for a, b in zip((h, qs, ks), before))

    def some_units(count, which, before, fresh):
        if fresh:
            wds[...] = jnp.zeros_like(wds)

        def step(n, carry):
            return maybe_unit(*which(n), carry)

        return lax.fori_loop(0, count, step, before)

    scores(0, y, z, True)
    products(0, y, z)
    scores(1, z, y, True)
    pending = (jnp.int32(1), z, y)

    second = []
    for some in (("q", "k"), ("v",), ("do", "st")):
        for axis in (0, 1):
            for name in some:
                for d in (0, 1):
                    first[axis, d, name].wait_recv()
                    if d == (0 if name in ("q", "k") else 1):
                        step = 1 if d == 0 else -1
                        ref = item(axis, name, ring(axis, -step))
                        n = 5 + names.index(name)
                        c = remote(ref, ref, gs.at[axis, d, n], gr.at[axis, d, n], peer(axis, step))
                        c.start()
                        second.append(c)

    pending = some_units(16, lambda n: (n // 8, (n % 8 + 1) // 3, (n % 8 + 1) % 3), pending, False)
    for c in second:
        c.wait_recv()

    class Reduction:
        def __init__(self, tx, rx, axis, base, get):
            self.tx, self.rx, self.axis, self.base, self.get = tx, rx, axis, base, get
            self.out = {}

        def go(self, j, value, step):
            axis = self.axis
            self.tx[axis, j] = value.astype(BF16)
            c = remote(
                self.tx.at[axis, j], self.rx.at[axis, j],
                rs.at[axis, self.base + j], rr.at[axis, self.base + j], peer(axis, step),
            )
            c.start()
            self.out[j] = c

        def far(self):
            slot = ring(self.axis, 2)
            self.go(0, self.get(slot, 0), 1)
            self.go(1, self.get(slot, 1), -1)

        def direct(self):
            self.go(2, self.get(ring(self.axis, 1), 1), 1)
            self.go(3, self.get(ring(self.axis, -1), 0), -1)

        def summed(self):
            for j, step in ((0, 1), (1, -1)):
                mine = self.get(ring(self.axis, step), j)
                self.out[j].wait_recv()
                self.go(4 + j, mine + self.rx[self.axis, j].astype(F32), step)

        def end(self):
            own0 = self.get(pos[self.axis], 0)
            own1 = self.get(pos[self.axis], 1)
            for j in (2, 3, 4, 5):
                self.out[j].wait_recv()
            rx = self.rx
            r0 = own0 + rx[self.axis, 3].astype(F32) + rx[self.axis, 4].astype(F32)
            r1 = own1 + rx[self.axis, 2].astype(F32) + rx[self.axis, 5].astype(F32)
            return r0, r1

        def drain(self):
            for c in self.out.values():
                c.wait_send()

    def get_dq(h):
        return lambda slot, p: dqt[h, slot, 64 * p : 64 * p + 64] * SCALE

    def get_dkv(h):
        return lambda slot, p: dkv[h, slot, p] * (SCALE if p == 0 else 1.0)

    def get_wg(h):
        def get(slot, p):
            parts = []
            for o in (2 * p, 2 * p + 1):
                blk = o * 4 + slot if h == 0 else slot * 4 + o
                cols = lat[:, pl.ds(pl.multiple_of(blk * T, T), T)]
                parts.append(dot(dqf[h], cols))
            return jnp.stack(parts)

        return get

    def get_last(h):
        def get(slot, p):
            start = pl.multiple_of(slot * 128 + 64 * p, 64)
            return jnp.concatenate(
                [wide[h, pl.ds(start, 64), :], wide[2 + h, pl.ds(start, 64), :]], axis=1
            )

        return get

    both = (0, 1)
    dq = [Reduction(qtx, qrx, h, 0, get_dq(h)) for h in both]
    dk = [Reduction(ktx, krx, 1 - h, 18, get_dkv(h)) for h in both]
    wa = [Reduction(atx, arx, h, 6, get_wg(h)) for h in both]
    wb = [Reduction(btx, brx, 1 - h, 12, get_last(h)) for h in both]

    pending = some_units(8, lambda n: (n // 4, jnp.int32(3), n % 4), pending, False)
    products(*pending)
    for h in both:
        dq[h].far()
    for h in both:
        dk[h].direct()
    pending = some_units(6, lambda n: (n // 3, n % 3, jnp.int32(3)), pending, True)
    products(*pending)
    for h in both:
        dq[h].direct()
    for h in both:
        dq[h].summed()
    for h in both:
        dk[h].far()
    for h in both:
        dk[h].summed()
    loads[8].wait()
    for h in both:
        r0, r1 = dq[h].end()
        dqf[h, 0:64] = r0.astype(BF16)
        dqf[h, 64:128] = r1.astype(BF16)
        wa[h].far()
    for h in both:
        wa[h].direct()
    for h in both:
        wa[h].summed()
    for h in both:
        wide2[pl.ds(h, T, stride=2), :] = jnp.transpose(dqf[h].astype(F32))
    qg_ref[...] = wide2[0 : 2 * T, :].astype(BF16)
    for h in both:
        r0, r1 = wa[h].end()
        for o in range(4):
            part = r0[o] if o < 2 else r1[o - 2]
            wide[h, pl.ds(o * 128, 128), :] = part[:, 0:128]
            wide[2 + h, pl.ds(o * 128, 128), :] = part[:, 128:256]
        wb[h].far()
        wb[h].direct()
    for h in both:
        wb[h].summed()
    for p, ref in ((0, kg_ref), (1, vg_ref)):
        for h in both:
            if p == 0:
                ends = dk[h].end()
                dk[h].ends = ends
            wide2[pl.ds(2 * T * p + h, T, stride=2), :] = dk[h].ends[p]
        ref[...] = wide2[2 * T * p : 2 * T * p + 2 * T, :].astype(BF16)
    for h in both:
        r0, r1 = wb[h].end()
        wg_ref[:, h * W : h * W + W] = jnp.transpose(jnp.concatenate([r0, r1], axis=0))

    for c in first.values():
        c.wait_send()
    for c in second:
        c.wait_send()
    for group in (dq, dk, wa, wb):
        for r in group:
            r.drain()


def put_kernel(*refs):
    sems = refs[8]
    copies = [pltpu.make_async_copy(refs[n], refs[4 + n], sems.at[n]) for n in range(4)]
    for c in copies:
        c.start()
    for c in copies:
        c.wait()


def body(latents, query_heads, key_heads, value_heads, map_outputs, log_sums, out_grad, mix_lambda, norm_gain):
    rows = 2 * T
    hbm = pl.BlockSpec(memory_space=pltpu.HBM)
    vmem = pl.BlockSpec(memory_space=pltpu.VMEM)
    out_shape = (
        jax.ShapeDtypeStruct((rows, W), BF16),
        jax.ShapeDtypeStruct((rows, W), BF16),
        jax.ShapeDtypeStruct((rows, W), BF16),
        jax.ShapeDtypeStruct((T, 2 * W), F32),
    )
    outs = pl.pallas_call(
        kernel,
        out_shape=tuple(pltpu.VMEM(o.shape, o.dtype) for o in out_shape),
        in_specs=[hbm] * 9,
        out_specs=(vmem, vmem, vmem, vmem),
        scratch_shapes=[
            pltpu.VMEM((rows, W), BF16),
            pltpu.VMEM((rows, W), BF16),
            pltpu.VMEM((rows, W), BF16),
            pltpu.VMEM((2 * rows, W), BF16),
            pltpu.VMEM((2, 2, T), F32),
            pltpu.VMEM((rows, W), BF16),
            pltpu.SMEM((2,), F32),
            pltpu.VMEM((1, W), F32),
            pltpu.VMEM((T, 4096), BF16),
            pltpu.VMEM((2, 4, 2, T, W), BF16),
            pltpu.VMEM((2, 4, 2, T, W), BF16),
            pltpu.VMEM((2, 4, 8, T), F32),
            pltpu.VMEM((2, 4, W, T), F32),
            pltpu.VMEM((2, 4, 2, T, W), F32),
            pltpu.VMEM((3, T, T), BF16),
            pltpu.VMEM((4, rows, W), F32),
            pltpu.VMEM((4 * T, W), F32),
            pltpu.VMEM((2, W, T), BF16),
            pltpu.VMEM((2, 6, 64, T), BF16),
            pltpu.VMEM((2, 6, 64, T), BF16),
            pltpu.VMEM((2, 6, T, W), BF16),
            pltpu.VMEM((2, 6, T, W), BF16),
            pltpu.VMEM((2, 6, 2, W, T), BF16),
            pltpu.VMEM((2, 6, 2, W, T), BF16),
            pltpu.VMEM((2, 6, 64, T), BF16),
            pltpu.VMEM((2, 6, 64, T), BF16),
            pltpu.SemaphoreType.DMA((9,)),
            pltpu.SemaphoreType.DMA((2, 2, 10)),
            pltpu.SemaphoreType.DMA((2, 2, 10)),
            pltpu.SemaphoreType.DMA((2, 24)),
            pltpu.SemaphoreType.DMA((2, 24)),
        ],
        compiler_params=pltpu.CompilerParams(
            collective_id=0, has_side_effects=True, vmem_limit_bytes=VMEM_ALL
        ),
    )(
        query_heads.reshape(rows, W),
        key_heads.reshape(rows, W),
        value_heads.reshape(rows, W),
        map_outputs.reshape(2 * rows, W),
        jnp.transpose(log_sums, (1, 2, 0)),
        out_grad.reshape(rows, W),
        mix_lambda,
        norm_gain.reshape(1, W),
        latents,
    )
    qg, kg, vg, wg = pl.pallas_call(
        put_kernel,
        out_shape=out_shape,
        in_specs=[vmem] * 4,
        out_specs=(hbm, hbm, hbm, hbm),
        scratch_shapes=[pltpu.SemaphoreType.DMA((4,))],
        compiler_params=pltpu.CompilerParams(vmem_limit_bytes=1024 * 1024),
    )(*outs)
    shape = query_heads.shape
    return (qg.reshape(shape), kg.reshape(shape), vg.reshape(shape), wg)


def solution(mesh):
    placed = (
        P("sp", None),
        P("sp", "tp", None),
        P("sp", "tp", None),
        P("sp", "tp", None),
        P("sp", None, "tp", None),
        P("sp", "tp", None),
        P("sp", "tp", None),
        P("tp"),
        P(),
    )
    return jax.shard_map(
        body,
        mesh=mesh,
        in_specs=placed,
        out_specs=(P("sp", "tp", None), P("sp", "tp", None), P("sp", "tp", None), P("sp", "tp")),
        check_vma=False,
    )
```

```python
import functools

import jax
import jax.numpy as jnp
from jax import lax
from jax.experimental import pallas as pl
from jax.experimental.pallas import tpu as pltpu
from jax.sharding import PartitionSpec as P

F32 = jnp.float32
BF16 = jnp.bfloat16
EPSILON = 1e-05
LOG2E = 1.4426950408889634
SCALE = 0.125
T = 256
W = 128
VMEM_ALL = 66200000
NT = (((1,), (1,)), ((), ()))


def dot(a, b):
    return jnp.dot(a, b, preferred_element_type=F32)


def dot_nt(a, b):
    return lax.dot_general(a, b, NT, preferred_element_type=F32)


def kernel(
    q_hbm, k_hbm, v_hbm, mo_hbm, lse_hbm, og_hbm, lam_hbm, gain_hbm, lat_hbm,
    qg_ref, kg_ref, vg_ref, wg_ref,
    q_in, k_in, v_in, mo_in, lse_in, og_in, lam_in, gain_in,
    lat, lx, qdo, kv, st, dqt, dkv, wds, wide, wide2, dqf, dqg,
    qtx, qrx, ktx, krx, etx, erx, btx, brx,
    in_sem, gs, gr, rs, rr, ls, lr, ds, dr, hs, hr, es, er,
):
    sp = lax.axis_index("sp")
    tp = lax.axis_index("tp")
    z = sp // 4
    y = sp % 4
    pos = (y, z)

    def ring(axis, step):
        return lax.rem(pos[axis] + step + 4, 4)

    def peer(axis, step):
        moved = ring(axis, step)
        return (z * 4 + moved if axis == 0 else moved * 4 + y, tp)

    def remote(src, dst, send, recv, device):
        return pltpu.make_async_remote_copy(
            src_ref=src, dst_ref=dst, send_sem=send, recv_sem=recv,
            device_id=device, device_id_type=pl.DeviceIdType.MESH,
        )

    def role_step(axis, role):
        sign = 1 - 2 * (pos[axis] % 2)
        return sign if role == 0 else -sign

    core = tp % 2
    sibling = (sp, tp + 1 - 2 * core)
    barrier = pltpu.get_barrier_semaphore()
    pl.semaphore_signal(barrier, inc=1, device_id=sibling, device_id_type=pl.DeviceIdType.MESH)
    for axis in (0, 1):
        for step in (1, -1):
            pl.semaphore_signal(
                barrier, inc=1, device_id=peer(axis, step), device_id_type=pl.DeviceIdType.MESH
            )
    sources = (q_hbm, k_hbm, v_hbm, og_hbm, mo_hbm, lse_hbm, lam_hbm, gain_hbm)
    targets = (q_in, k_in, v_in, og_in, mo_in, lse_in, lam_in, gain_in)
    loads = [pltpu.make_async_copy(a, b, in_sem.at[n]) for n, (a, b) in enumerate(zip(sources, targets))]
    loads += [
        pltpu.make_async_copy(lat_hbm.at[:, n * T : n * T + T], lat.at[n // 4, n % 4], in_sem.at[8 + n])
        for n in range(16)
    ]
    for c in loads:
        c.start()

    qpos = (y, z)
    kpos = (z, y)
    for n, ref in enumerate((q_in, k_in, v_in)):
        loads[n].wait()
        wide[n] = ref[...].astype(F32)
    for h in (0, 1):
        qdo[h, qpos[h], 0] = wide[0, pl.ds(h, T, stride=2), :].astype(BF16)
        kv[h, kpos[h], 0] = wide[1, pl.ds(h, T, stride=2), :].astype(BF16)
        kv[h, kpos[h], 1] = wide[2, pl.ds(h, T, stride=2), :].astype(BF16)
    pl.semaphore_wait(barrier, 5)

    qh = (0, 1)
    kh = (1, 0)
    first = {}

    def item(axis, name, slot):
        if name == "q":
            return qdo.at[qh[axis], slot, 0]
        if name == "do":
            return qdo.at[qh[axis], slot, 1]
        if name == "st":
            return st.at[qh[axis], slot]
        if name == "k":
            return kv.at[kh[axis], slot, 0]
        return kv.at[kh[axis], slot, 1]

    names = ("q", "k", "v", "do", "st")

    def send_own(some):
        for name in some:
            for axis in (0, 1):
                for d, step in enumerate((1, -1)):
                    n = names.index(name)
                    ref = item(axis, name, pos[axis])
                    c = remote(ref, ref, gs.at[axis, d, n], gr.at[axis, d, n], peer(axis, step))
                    c.start()
                    first[axis, d, name] = c

    send_own(("q", "k", "v"))

    for c in loads[3:8]:
        c.wait()
    wide[3] = og_in[...].astype(F32)
    wide2[...] = mo_in[...].astype(F32)
    gain = gain_in[...]
    for h in (0, 1):
        lam = lam_in[h]
        m1 = wide2[pl.ds(h, T, stride=4), :]
        m2 = wide2[pl.ds(2 + h, T, stride=4), :]
        comb = m1 - lam * m2
        inv = lax.rsqrt(jnp.mean(comb * comb, axis=-1, keepdims=True) + EPSILON)
        wtd = gain * wide[3, pl.ds(h, T, stride=2), :]
        cross = jnp.mean(comb * wtd, axis=-1, keepdims=True)
        grad = (inv * wtd - inv * inv * inv * comb * cross).astype(BF16)
        qdo[h, qpos[h], 1] = grad
        gf = grad.astype(F32)
        r1 = jnp.sum(jnp.transpose(gf * m1), axis=0, keepdims=True)
        r2 = jnp.sum(jnp.transpose(gf * m2), axis=0, keepdims=True)
        lam_row = jnp.full((1, T), lam, F32)
        st[h, qpos[h], 0:1] = lse_in[h, 0:1, :] * LOG2E
        st[h, qpos[h], 1:2] = (lse_in[h, 1:2, :] - jnp.log(lam_row)) * LOG2E
        st[h, qpos[h], 2:3] = r1
        st[h, qpos[h], 3:4] = r2
        st[h, qpos[h], 4:8] = jnp.zeros((4, T), F32)
    send_own(("do", "st"))

    dqt[...] = jnp.zeros_like(dqt)
    dkv[...] = jnp.zeros_like(dkv)

    lane = lax.broadcasted_iota(jnp.int32, (T, W), 1)

    def split_queries(h, qs):
        q = qdo[h, qs, 0]
        zero = jnp.zeros_like(q)
        return jnp.where(lane < 64, q, zero), jnp.where(lane < 64, zero, -q)

    def scores(h, qs, ks, masked):
        q1, q2 = split_queries(h, qs)
        do = qdo[h, qs, 1]
        half = T // 2
        for c in (0, half):
            k = kv[h, ks, 0, c : c + half]
            v = kv[h, ks, 1, c : c + half]
            s1 = dot_nt(k, q1)
            s2 = dot_nt(k, q2)
            dp = dot_nt(v, do)
            p1 = jnp.exp2(s1 * (SCALE * LOG2E) - st[h, qs, 0:1])
            p2 = jnp.exp2(s2 * (-SCALE * LOG2E) - st[h, qs, 1:2])
            if masked:
                rows = lax.broadcasted_iota(jnp.int32, (half, T), 0) + c
                cols = lax.broadcasted_iota(jnp.int32, (half, T), 1)
                keep = rows <= cols
                p1 = jnp.where(keep, p1, 0.0)
                p2 = jnp.where(keep, p2, 0.0)
            wds[0, c : c + half] = (p1 - p2).astype(BF16)
            wds[1, c : c + half] = (p1 * (dp - st[h, qs, 2:3])).astype(BF16)
            wds[2, c : c + half] = (p2 * (dp - st[h, qs, 3:4])).astype(BF16)

    def products(h, qs, ks):
        q1, q2 = split_queries(h, qs)
        w, d1, d2 = wds[0], wds[1], wds[2]
        kt = jnp.transpose(kv[h, ks, 0])
        dqt[h, qs, 0:64] += dot(kt[0:64], d1)
        dqt[h, qs, 64:128] -= dot(kt[64:128], d2)
        dkv[h, ks, 0] += dot(d1, q1) + dot(d2, q2)
        dkv[h, ks, 1] += dot(w, qdo[h, qs, 1])

    def maybe_unit(h, i, j, before):
        qo = jnp.where(i < 2, i, 5 - i)
        ko = jnp.where(j < 2, j, 5 - j)
        qbase = jnp.where(h == 0, y, z)
        kbase = jnp.where(h == 0, z, y)
        qs = (qbase + qo) % 4
        ks = (kbase + ko) % 4
        q_block = jnp.where(h == 0, z * 4 + qs, qs * 4 + y)
        k_block = jnp.where(h == 0, ks * 4 + y, z * 4 + ks)
        wanted = k_block < q_block

        @pl.when(wanted)
        def _():
            products(*before)
            scores(h, qs, ks, False)

        return tuple(jnp.where(wanted, a, b) for a, b in zip((h, qs, ks), before))

    def some_units(count, which, before, fresh):
        if fresh:
            wds[...] = jnp.zeros_like(wds)

        def step(n, carry):
            return maybe_unit(*which(n), carry)

        return lax.fori_loop(0, count, step, before)

    scores(0, y, z, True)
    products(0, y, z)
    scores(1, z, y, True)
    pending = (jnp.int32(1), z, y)

    second = []
    for some in (("q", "k"), ("v",), ("do", "st")):
        for axis in (0, 1):
            for name in some:
                for d in (0, 1):
                    first[axis, d, name].wait_recv()
                    if d == (0 if name in ("q", "k") else 1):
                        step = 1 if d == 0 else -1
                        ref = item(axis, name, ring(axis, -step))
                        n = 5 + names.index(name)
                        c = remote(ref, ref, gs.at[axis, d, n], gr.at[axis, d, n], peer(axis, step))
                        c.start()
                        second.append(c)

    for c in loads[8:]:
        c.wait()
    rows = pl.ds(pl.multiple_of(core * 128, 128), 128)
    shares = []
    for axis in (0, 1):
        for role in (0, 1):
            step = role_step(axis, role)
            for w, owner in enumerate((ring(axis, step), ring(axis, 2))):
                some = slice(2 * role, 2 * role + 2)
                src = lat.at[some, owner, rows, :] if axis == 0 else lat.at[owner, some, rows, :]
                c = remote(
                    src, lx.at[axis, role, w, :, rows, :], ls.at[axis, role, w], lr.at[axis, role, w],
                    peer(axis, step),
                )
                c.start()
                shares.append(c)

    pending = some_units(16, lambda n: (n // 8, (n % 8 + 1) // 3, (n % 8 + 1) % 3), pending, False)
    for c in second:
        c.wait_recv()

    class Reduction:
        def __init__(self, tx, rx, axis, base, get):
            self.tx, self.rx, self.axis, self.base, self.get = tx, rx, axis, base, get
            self.out = {}

        def go(self, j, value, step):
            axis = self.axis
            self.tx[axis, j] = value.astype(BF16)
            c = remote(
                self.tx.at[axis, j], self.rx.at[axis, j],
                rs.at[axis, self.base + j], rr.at[axis, self.base + j], peer(axis, step),
            )
            c.start()
            self.out[j] = c

        def far(self):
            slot = ring(self.axis, 2)
            self.go(0, self.get(slot, 0), 1)
            self.go(1, self.get(slot, 1), -1)

        def direct(self):
            self.go(2, self.get(ring(self.axis, 1), 1), 1)
            self.go(3, self.get(ring(self.axis, -1), 0), -1)

        def summed(self):
            for j, step in ((0, 1), (1, -1)):
                mine = self.get(ring(self.axis, step), j)
                self.out[j].wait_recv()
                self.go(4 + j, mine + self.rx[self.axis, j].astype(F32), step)

        def end(self):
            own0 = self.get(pos[self.axis], 0)
            own1 = self.get(pos[self.axis], 1)
            for j in (2, 3, 4, 5):
                self.out[j].wait_recv()
            rx = self.rx
            r0 = own0 + rx[self.axis, 3].astype(F32) + rx[self.axis, 4].astype(F32)
            r1 = own1 + rx[self.axis, 2].astype(F32) + rx[self.axis, 5].astype(F32)
            return r0, r1

        def drain(self):
            for c in self.out.values():
                c.wait_send()

    def get_dq(h):
        return lambda slot, p: dqt[h, slot, 64 * p : 64 * p + 64] * SCALE

    def get_dkv(h):
        return lambda slot, p: dkv[h, slot, p] * (SCALE if p == 0 else 1.0)

    def get_last(h):
        def get(slot, p):
            start = pl.multiple_of(slot * 128 + 64 * p, 64)
            return jnp.concatenate(
                [wide[h, pl.ds(start, 64), :], wide[2 + h, pl.ds(start, 64), :]], axis=1
            )

        return get

    both = (0, 1)
    dq = [Reduction(qtx, qrx, h, 0, get_dq(h)) for h in both]
    dk = [Reduction(ktx, krx, 1 - h, 18, get_dkv(h)) for h in both]
    wb = [Reduction(btx, brx, 1 - h, 12, get_last(h)) for h in both]

    pending = some_units(8, lambda n: (n // 4, jnp.int32(3), n % 4), pending, False)
    products(*pending)
    for h in both:
        dq[h].far()
    for h in both:
        dk[h].direct()
    pending = some_units(6, lambda n: (n // 3, n % 3, jnp.int32(3)), pending, True)
    products(*pending)
    for h in both:
        dq[h].direct()
    for h in both:
        dq[h].summed()
    for h in both:
        dk[h].far()
    def block(h, owner, o):
        return lat[o, owner] if h == 0 else lat[owner, o]

    def term(h, role, w, owner, o):
        near = dot(dqf[h], block(h, owner, 2 * role + o))
        return near + dot(dqg[h, role], lx[h, role, w, o])

    hands = {}
    for h in both:
        r0, r1 = dq[h].end()
        dqf[h, 0:64] = r0.astype(BF16)
        dqf[h, 64:128] = r1.astype(BF16)
        for role in both:
            c = remote(
                dqf.at[h], dqg.at[h, role], hs.at[h, role], hr.at[h, role], peer(h, role_step(h, role))
            )
            c.start()
            hands[h, role] = c
    swaps = []
    for c in shares:
        c.wait_recv()
    for axis in (0, 1):
        for role in (0, 1):
            ref = lx.at[axis, role, :, :, rows, :]
            c = remote(ref, ref, ds.at[axis, role], dr.at[axis, role], sibling)
            c.start()
            swaps.append(c)
    for h in both:
        dk[h].summed()
    for c in swaps:
        c.wait_recv()
    odd = [pos[1 - h] % 2 for h in both]
    trades = {}
    for h in both:
        for role in both:
            step = role_step(h, 1 - role)
            hands[h, role].wait_recv()
            for n, o in enumerate((odd[h], 1 - odd[h])):
                etx[h, role, n] = term(h, role, 1, ring(h, step), o).astype(BF16)
                c = remote(
                    etx.at[h, role, n], erx.at[h, role, n], es.at[h, role, n], er.at[h, role, n],
                    peer(h, step),
                )
                c.start()
                trades[h, role, n] = c

    def place(h, slot):
        return pl.ds(pl.multiple_of(slot * 128, 128), 128)

    for h in both:
        for role in both:
            for o in both:
                part = term(h, role, 0, pos[h], o)
                wide[h, place(h, 2 * role + o), :] = part[:, 0:128]
                wide[2 + h, place(h, 2 * role + o), :] = part[:, 128:256]
    for h in both:
        wide2[pl.ds(h, T, stride=2), :] = jnp.transpose(dqf[h].astype(F32))
    qg_ref[...] = wide2[0 : 2 * T, :].astype(BF16)
    ends = [dk[h].end() for h in both]
    for p, ref in ((0, kg_ref), (1, vg_ref)):
        for h in both:
            wide2[pl.ds(2 * T * p + h, T, stride=2), :] = ends[h][p]
        ref[...] = wide2[2 * T * p : 2 * T * p + 2 * T, :].astype(BF16)
    for n in both:
        for h in both:
            o = odd[h] if n == 0 else 1 - odd[h]
            for role in both:
                trades[h, role, n].wait_recv()
                got = erx[h, role, n].astype(F32)
                wide[h, place(h, 2 * role + o), :] += got[:, 0:128]
                wide[2 + h, place(h, 2 * role + o), :] += got[:, 128:256]
            if n == 0:
                wb[h].far()
            else:
                wb[h].direct()
    for h in both:
        wb[h].summed()
    for h in both:
        r0, r1 = wb[h].end()
        wg_ref[:, h * W : h * W + W] = jnp.transpose(jnp.concatenate([r0, r1], axis=0))

    for c in first.values():
        c.wait_send()
    for c in second:
        c.wait_send()
    for c in shares + swaps + list(hands.values()) + list(trades.values()):
        c.wait_send()
    for group in (dq, dk, wb):
        for r in group:
            r.drain()


def put_kernel(*refs):
    sems = refs[8]
    copies = [pltpu.make_async_copy(refs[n], refs[4 + n], sems.at[n]) for n in range(4)]
    for c in copies:
        c.start()
    for c in copies:
        c.wait()


def body(latents, query_heads, key_heads, value_heads, map_outputs, log_sums, out_grad, mix_lambda, norm_gain):
    rows = 2 * T
    hbm = pl.BlockSpec(memory_space=pltpu.HBM)
    vmem = pl.BlockSpec(memory_space=pltpu.VMEM)
    out_shape = (
        jax.ShapeDtypeStruct((rows, W), BF16),
        jax.ShapeDtypeStruct((rows, W), BF16),
        jax.ShapeDtypeStruct((rows, W), BF16),
        jax.ShapeDtypeStruct((T, 2 * W), F32),
    )
    outs = pl.pallas_call(
        kernel,
        out_shape=tuple(pltpu.VMEM(o.shape, o.dtype) for o in out_shape),
        in_specs=[hbm] * 9,
        out_specs=(vmem, vmem, vmem, vmem),
        scratch_shapes=[
            pltpu.VMEM((rows, W), BF16),
            pltpu.VMEM((rows, W), BF16),
            pltpu.VMEM((rows, W), BF16),
            pltpu.VMEM((2 * rows, W), BF16),
            pltpu.VMEM((2, 2, T), F32),
            pltpu.VMEM((rows, W), BF16),
            pltpu.SMEM((2,), F32),
            pltpu.VMEM((1, W), F32),
            pltpu.VMEM((4, 4, T, T), BF16),
            pltpu.VMEM((2, 2, 2, 2, T, T), BF16),
            pltpu.VMEM((2, 4, 2, T, W), BF16),
            pltpu.VMEM((2, 4, 2, T, W), BF16),
            pltpu.VMEM((2, 4, 8, T), F32),
            pltpu.VMEM((2, 4, W, T), F32),
            pltpu.VMEM((2, 4, 2, T, W), F32),
            pltpu.VMEM((3, T, T), BF16),
            pltpu.VMEM((4, rows, W), F32),
            pltpu.VMEM((4 * T, W), F32),
            pltpu.VMEM((2, W, T), BF16),
            pltpu.VMEM((2, 2, W, T), BF16),
            pltpu.VMEM((2, 6, 64, T), BF16),
            pltpu.VMEM((2, 6, 64, T), BF16),
            pltpu.VMEM((2, 6, T, W), BF16),
            pltpu.VMEM((2, 6, T, W), BF16),
            pltpu.VMEM((2, 2, 2, W, T), BF16),
            pltpu.VMEM((2, 2, 2, W, T), BF16),
            pltpu.VMEM((2, 6, 64, T), BF16),
            pltpu.VMEM((2, 6, 64, T), BF16),
            pltpu.SemaphoreType.DMA((24,)),
            pltpu.SemaphoreType.DMA((2, 2, 10)),
            pltpu.SemaphoreType.DMA((2, 2, 10)),
            pltpu.SemaphoreType.DMA((2, 24)),
            pltpu.SemaphoreType.DMA((2, 24)),
            pltpu.SemaphoreType.DMA((2, 2, 2)),
            pltpu.SemaphoreType.DMA((2, 2, 2)),
            pltpu.SemaphoreType.DMA((2, 2)),
            pltpu.SemaphoreType.DMA((2, 2)),
            pltpu.SemaphoreType.DMA((2, 2)),
            pltpu.SemaphoreType.DMA((2, 2)),
            pltpu.SemaphoreType.DMA((2, 2, 2)),
            pltpu.SemaphoreType.DMA((2, 2, 2)),
        ],
        compiler_params=pltpu.CompilerParams(
            collective_id=0, has_side_effects=True, vmem_limit_bytes=VMEM_ALL
        ),
    )(
        query_heads.reshape(rows, W),
        key_heads.reshape(rows, W),
        value_heads.reshape(rows, W),
        map_outputs.reshape(2 * rows, W),
        jnp.transpose(log_sums, (1, 2, 0)),
        out_grad.reshape(rows, W),
        mix_lambda,
        norm_gain.reshape(1, W),
        latents,
    )
    qg, kg, vg, wg = pl.pallas_call(
        put_kernel,
        out_shape=out_shape,
        in_specs=[vmem] * 4,
        out_specs=(hbm, hbm, hbm, hbm),
        scratch_shapes=[pltpu.SemaphoreType.DMA((4,))],
        compiler_params=pltpu.CompilerParams(vmem_limit_bytes=1024 * 1024),
    )(*outs)
    shape = query_heads.shape
    return (qg.reshape(shape), kg.reshape(shape), vg.reshape(shape), wg)


def solution(mesh):
    placed = (
        P("sp", None),
        P("sp", "tp", None),
        P("sp", "tp", None),
        P("sp", "tp", None),
        P("sp", None, "tp", None),
        P("sp", "tp", None),
        P("sp", "tp", None),
        P("tp"),
        P(),
    )
    return jax.shard_map(
        body,
        mesh=mesh,
        in_specs=placed,
        out_specs=(P("sp", "tp", None), P("sp", "tp", None), P("sp", "tp", None), P("sp", "tp")),
        check_vma=False,
    )
```

```python
import functools

import jax
import jax.numpy as jnp
from jax import lax
from jax.experimental import pallas as pl
from jax.experimental.pallas import tpu as pltpu
from jax.sharding import PartitionSpec as P

F32 = jnp.float32
BF16 = jnp.bfloat16
EPSILON = 1e-05
LOG2E = 1.4426950408889634
SCALE = 0.125
T = 256
W = 128
VMEM_ALL = 66200000
NT = (((1,), (1,)), ((), ()))


def dot(a, b):
    return jnp.dot(a, b, preferred_element_type=F32)


def dot_nt(a, b):
    return lax.dot_general(a, b, NT, preferred_element_type=F32)


def kernel(
    q_hbm, k_hbm, v_hbm, mo_hbm, lse_hbm, og_hbm, lam_hbm, gain_hbm, lat_hbm,
    qg_ref, kg_ref, vg_ref, wg_ref,
    q_in, k_in, v_in, mo_in, lse_in, og_in, lam_in, gain_in,
    lat, lx, qdo, kv, st, dqt, dkv, wds, wide, wide2, dqf, dqg,
    qtx, qrx, ktx, krx, etx, erx, btx, brx, pre,
    in_sem, gs, gr, rs, rr, ls, lr, ds, dr, hs, hr, es, er,
):
    sp = lax.axis_index("sp")
    tp = lax.axis_index("tp")
    z = sp // 4
    y = sp % 4
    pos = (y, z)

    def ring(axis, step):
        return lax.rem(pos[axis] + step + 4, 4)

    def peer(axis, step):
        moved = ring(axis, step)
        return (z * 4 + moved if axis == 0 else moved * 4 + y, tp)

    def remote(src, dst, send, recv, device):
        return pltpu.make_async_remote_copy(
            src_ref=src, dst_ref=dst, send_sem=send, recv_sem=recv,
            device_id=device, device_id_type=pl.DeviceIdType.MESH,
        )

    def role_step(axis, role):
        sign = 1 - 2 * (pos[axis] % 2)
        return sign if role == 0 else -sign

    core = tp % 2
    sibling = (sp, tp + 1 - 2 * core)
    barrier = pltpu.get_barrier_semaphore()
    pl.semaphore_signal(barrier, inc=1, device_id=sibling, device_id_type=pl.DeviceIdType.MESH)
    for axis in (0, 1):
        for step in (1, -1, 2):
            pl.semaphore_signal(
                barrier, inc=1, device_id=peer(axis, step), device_id_type=pl.DeviceIdType.MESH
            )
    sources = (q_hbm, k_hbm, v_hbm, og_hbm, mo_hbm, lse_hbm, lam_hbm, gain_hbm)
    targets = (q_in, k_in, v_in, og_in, mo_in, lse_in, lam_in, gain_in)
    loads = [pltpu.make_async_copy(a, b, in_sem.at[n]) for n, (a, b) in enumerate(zip(sources, targets))]
    loads += [
        pltpu.make_async_copy(lat_hbm.at[:, n * T : n * T + T], lat.at[n // 4, n % 4], in_sem.at[8 + n])
        for n in range(16)
    ]
    for c in loads:
        c.start()

    qpos = (y, z)
    kpos = (z, y)
    qh = (0, 1)
    kh = (1, 0)
    first = {}

    def item(axis, name, slot):
        if name == "q":
            return qdo.at[qh[axis], slot, 0]
        if name == "do":
            return qdo.at[qh[axis], slot, 1]
        if name == "st":
            return st.at[qh[axis], slot]
        if name == "k":
            return kv.at[kh[axis], slot, 0]
        return kv.at[kh[axis], slot, 1]

    names = ("q", "k", "v", "do", "st")

    def gather_copy(axis, d, name, slot, forward):
        n = names.index(name) + (5 if forward else 0)
        ref = item(axis, name, slot)
        step = 1 if d == 0 else -1
        return remote(ref, ref, gs.at[axis, d, n], gr.at[axis, d, n], peer(axis, step))

    ups = ("k", "v")
    downs = ("q", "do", "st")

    def z_each(some, forward, do_it):
        if forward:
            middle = (z == 1) | (z == 2)
            cases = ((0, middle, ups, -1), (1, middle, downs, 1))
        else:
            cases = ((0, z < 3, ups, 0), (0, z == 3, downs, 0), (1, z > 0, downs, 0), (1, z == 0, ups, 0))
        for d, wanted, group, shift in cases:
            mine = [name for name in some if name in group]
            if mine:
                @pl.when(wanted)
                def _():
                    for name in mine:
                        do_it(gather_copy(1, d, name, ring(1, shift), forward))

    def z_arrived(some, forward):
        if forward:
            cases = ((0, z >= 2, ups, 2), (1, z < 2, downs, 2))
        else:
            cases = ((0, z > 0, ups, -1), (0, z == 0, downs, -1), (1, z < 3, downs, 1), (1, z == 3, ups, 1))
        for d, wanted, group, shift in cases:
            mine = [name for name in some if name in group]
            if mine:
                @pl.when(wanted)
                def _():
                    for name in mine:
                        gather_copy(1, d, name, ring(1, shift), forward).wait_recv()

    def start(c):
        c.start()

    def wait_send(c):
        c.wait_send()

    def send_own(some):
        for name in some:
            for d in (0, 1):
                c = gather_copy(0, d, name, y, False)
                c.start()
                first[d, name] = c
            z_each((name,), False, start)

    for n, (name, ref) in enumerate((("q", q_in), ("k", k_in), ("v", v_in))):
        loads[n].wait()
        wide[n] = ref[...].astype(F32)
        for h in (0, 1):
            part = wide[n, pl.ds(h, T, stride=2), :].astype(BF16)
            if n == 0:
                qdo[h, qpos[h], 0] = part
            else:
                kv[h, kpos[h], n - 1] = part
        if n == 0:
            pl.semaphore_wait(barrier, 7)
        send_own((name,))

    for c in loads[3:8]:
        c.wait()
    wide[3] = og_in[...].astype(F32)
    wide2[...] = mo_in[...].astype(F32)
    gain = gain_in[...]
    for h in (0, 1):
        lam = lam_in[h]
        m1 = wide2[pl.ds(h, T, stride=4), :]
        m2 = wide2[pl.ds(2 + h, T, stride=4), :]
        comb = m1 - lam * m2
        inv = lax.rsqrt(jnp.mean(comb * comb, axis=-1, keepdims=True) + EPSILON)
        wtd = gain * wide[3, pl.ds(h, T, stride=2), :]
        cross = jnp.mean(comb * wtd, axis=-1, keepdims=True)
        grad = (inv * wtd - inv * inv * inv * comb * cross).astype(BF16)
        qdo[h, qpos[h], 1] = grad
        gf = grad.astype(F32)
        r1 = jnp.sum(jnp.transpose(gf * m1), axis=0, keepdims=True)
        r2 = jnp.sum(jnp.transpose(gf * m2), axis=0, keepdims=True)
        lam_row = jnp.full((1, T), lam, F32)
        st[h, qpos[h], 0:1] = lse_in[h, 0:1, :] * LOG2E
        st[h, qpos[h], 1:2] = (lse_in[h, 1:2, :] - jnp.log(lam_row)) * LOG2E
        st[h, qpos[h], 2:3] = r1
        st[h, qpos[h], 3:4] = r2
        st[h, qpos[h], 4:8] = jnp.zeros((4, T), F32)
    send_own(("do", "st"))

    dqt[...] = jnp.zeros_like(dqt)
    dkv[...] = jnp.zeros_like(dkv)

    lane = lax.broadcasted_iota(jnp.int32, (T, W), 1)

    def split_queries(h, qs):
        q = qdo[h, qs, 0]
        zero = jnp.zeros_like(q)
        return jnp.where(lane < 64, q, zero), jnp.where(lane < 64, zero, -q)

    def scores(h, qs, ks, masked):
        q1, q2 = split_queries(h, qs)
        do = qdo[h, qs, 1]
        half = T // 2
        for c in (0, half):
            k = kv[h, ks, 0, c : c + half]
            v = kv[h, ks, 1, c : c + half]
            s1 = dot_nt(k, q1)
            s2 = dot_nt(k, q2)
            dp = dot_nt(v, do)
            p1 = jnp.exp2(s1 * (SCALE * LOG2E) - st[h, qs, 0:1])
            p2 = jnp.exp2(s2 * (-SCALE * LOG2E) - st[h, qs, 1:2])
            if masked:
                rows = lax.broadcasted_iota(jnp.int32, (half, T), 0) + c
                cols = lax.broadcasted_iota(jnp.int32, (half, T), 1)
                keep = rows <= cols
                p1 = jnp.where(keep, p1, 0.0)
                p2 = jnp.where(keep, p2, 0.0)
            wds[0, c : c + half] = (p1 - p2).astype(BF16)
            wds[1, c : c + half] = (p1 * (dp - st[h, qs, 2:3])).astype(BF16)
            wds[2, c : c + half] = (p2 * (dp - st[h, qs, 3:4])).astype(BF16)

    def products(h, qs, ks):
        q1, q2 = split_queries(h, qs)
        w, d1, d2 = wds[0], wds[1], wds[2]
        kt = jnp.transpose(kv[h, ks, 0])
        dqt[h, qs, 0:64] += dot(kt[0:64], d1)
        dqt[h, qs, 64:128] -= dot(kt[64:128], d2)
        dkv[h, ks, 0] += dot(d1, q1) + dot(d2, q2)
        dkv[h, ks, 1] += dot(w, qdo[h, qs, 1])

    def maybe_unit(h, i, j, before):
        qo = jnp.where(i < 2, i, 5 - i)
        ko = jnp.where(j < 2, j, 5 - j)
        qbase = jnp.where(h == 0, y, z)
        kbase = jnp.where(h == 0, z, y)
        qs = (qbase + qo) % 4
        ks = (kbase + ko) % 4
        q_block = jnp.where(h == 0, z * 4 + qs, qs * 4 + y)
        k_block = jnp.where(h == 0, ks * 4 + y, z * 4 + ks)
        wanted = k_block < q_block

        @pl.when(wanted)
        def _():
            products(*before)
            scores(h, qs, ks, False)

        return tuple(jnp.where(wanted, a, b) for a, b in zip((h, qs, ks), before))

    def some_units(count, which, before, fresh):
        if fresh:
            wds[...] = jnp.zeros_like(wds)

        def step(n, carry):
            return maybe_unit(*which(n), carry)

        return lax.fori_loop(0, count, step, before)

    scores(0, y, z, True)
    products(0, y, z)
    scores(1, z, y, True)
    pending = (jnp.int32(1), z, y)

    second = []
    for some in (("q", "k"), ("v",), ("do", "st")):
        for name in some:
            for d in (0, 1):
                first[d, name].wait_recv()
                if d == (0 if name in ("q", "k") else 1):
                    c = gather_copy(0, d, name, ring(0, -1 if d == 0 else 1), True)
                    c.start()
                    second.append(c)
        z_arrived(some, False)
        z_each(some, True, start)

    for c in loads[8:]:
        c.wait()
    rows = pl.ds(pl.multiple_of(core * 128, 128), 128)
    shares = []
    for axis in (0, 1):
        for role in (0, 1):
            step = role_step(axis, role)
            for w, owner in enumerate((ring(axis, step), ring(axis, 2))):
                some = slice(2 * role, 2 * role + 2)
                src = lat.at[some, owner, rows, :] if axis == 0 else lat.at[owner, some, rows, :]
                c = remote(
                    src, lx.at[axis, role, w, :, rows, :], ls.at[axis, role, w], lr.at[axis, role, w],
                    peer(axis, step),
                )
                c.start()
                shares.append(c)

    pending = some_units(16, lambda n: (n // 8, (n % 8 + 1) // 3, (n % 8 + 1) % 3), pending, False)
    z_arrived(names, True)
    pending = some_units(
        6, lambda n: (n // 3, jnp.where(n < 3, n, 3), jnp.where(n < 3, 3, n - 3)), pending, False
    )
    for c in second:
        c.wait_recv()

    class Reduction:
        def __init__(self, tx, rx, axis, base, get):
            self.tx, self.rx, self.axis, self.base, self.get = tx, rx, axis, base, get
            self.out = {}

        def go(self, j, value, step):
            axis = self.axis
            self.tx[axis, j] = value.astype(BF16)
            c = remote(
                self.tx.at[axis, j], self.rx.at[axis, j],
                rs.at[axis, self.base + j], rr.at[axis, self.base + j], peer(axis, step),
            )
            c.start()
            self.out[j] = c

        def far(self):
            slot = ring(self.axis, 2)
            self.go(0, self.get(slot, 0), 1)
            self.go(1, self.get(slot, 1), -1)

        def direct(self):
            self.go(2, self.get(ring(self.axis, 1), 1), 1)
            self.go(3, self.get(ring(self.axis, -1), 0), -1)

        def summed(self):
            for j, step in ((0, 1), (1, -1)):
                mine = self.get(ring(self.axis, step), j)
                self.out[j].wait_recv()
                self.go(4 + j, mine + self.rx[self.axis, j].astype(F32), step)

        def end(self):
            own0 = self.get(pos[self.axis], 0)
            own1 = self.get(pos[self.axis], 1)
            for j in (2, 3, 4, 5):
                self.out[j].wait_recv()
            rx = self.rx
            r0 = own0 + rx[self.axis, 3].astype(F32) + rx[self.axis, 4].astype(F32)
            r1 = own1 + rx[self.axis, 2].astype(F32) + rx[self.axis, 5].astype(F32)
            return r0, r1

        def drain(self):
            for c in self.out.values():
                c.wait_send()

    class Direct:
        def __init__(self, tx, rx, axis, base, get):
            self.tx, self.rx, self.axis, self.base, self.get = tx, rx, axis, base, get
            self.out = {}

        def go(self, j, step):
            axis = self.axis
            self.tx[axis, j] = self.get(ring(axis, step)).astype(BF16)
            c = remote(
                self.tx.at[axis, j], self.rx.at[axis, j],
                rs.at[axis, self.base + j], rr.at[axis, self.base + j], peer(axis, step),
            )
            c.start()
            self.out[j] = c

        def far(self):
            self.go(0, 2)

        def direct(self):
            self.go(1, 1)
            self.go(2, -1)

        def end(self):
            total = self.get(pos[self.axis])
            for j in (1, 2, 0):
                self.out[j].wait_recv()
                total = total + self.rx[self.axis, j].astype(F32)
            return total

        def drain(self):
            for c in self.out.values():
                c.wait_send()

    def get_dq(h):
        return lambda slot: dqt[h, slot] * SCALE

    def get_dkv(h):
        return lambda slot, p: dkv[h, slot, p] * (SCALE if p == 0 else 1.0)

    def get_last(h):
        def get(slot):
            rows = pl.ds(pl.multiple_of(slot * 128, 128), 128)
            return jnp.concatenate([wide[h, rows, :], wide[2 + h, rows, :]], axis=1)

        return get

    both = (0, 1)
    dq = [Direct(qtx, qrx, h, 0, get_dq(h)) for h in both]
    dk = [Reduction(ktx, krx, 1 - h, 18, get_dkv(h)) for h in both]
    wb = [Direct(btx, brx, 1 - h, 12, get_last(h)) for h in both]

    pending = some_units(
        5, lambda n: (jnp.where(n == 0, 1, 0), jnp.int32(3), jnp.where(n == 0, 3, n - 1)), pending, False
    )
    products(*pending)
    for h in both:
        dq[h].far()
    dq[0].direct()
    for h in both:
        dk[h].direct()
    pending = some_units(3, lambda n: (jnp.int32(1), n, jnp.int32(3)), pending, True)
    products(*pending)
    dq[1].direct()
    for h in both:
        dk[h].far()
    def block(h, owner, o):
        return lat[o, owner] if h == 0 else lat[owner, o]

    def term(h, role, w, owner, o):
        near = dot(dqf[h], block(h, owner, 2 * role + o))
        return near + dot(dqg[h, role], lx[h, role, w, o])

    hands = {}
    for h in both:
        dqf[h] = dq[h].end().astype(BF16)
        for role in both:
            c = remote(
                dqf.at[h], dqg.at[h, role], hs.at[h, role], hr.at[h, role], peer(h, role_step(h, role))
            )
            c.start()
            hands[h, role] = c
    swaps = []
    for c in shares:
        c.wait_recv()
    for axis in (0, 1):
        for role in (0, 1):
            ref = lx.at[axis, role, :, :, rows, :]
            c = remote(ref, ref, ds.at[axis, role], dr.at[axis, role], sibling)
            c.start()
            swaps.append(c)
    for h in both:
        dk[h].summed()
    for c in swaps:
        c.wait_recv()
    odd = [pos[1 - h] % 2 for h in both]
    trades = {}
    for h in both:
        for role in both:
            for n, o in enumerate((odd[h], 1 - odd[h])):
                pre[h, role, n] = dot(dqf[h], block(h, ring(h, role_step(h, 1 - role)), 2 * role + o))
    for n in both:
        for h in both:
            o = odd[h] if n == 0 else 1 - odd[h]
            for role in both:
                if n == 0:
                    hands[h, role].wait_recv()
                etx[h, role, n] = (pre[h, role, n] + dot(dqg[h, role], lx[h, role, 1, o])).astype(BF16)
                c = remote(
                    etx.at[h, role, n], erx.at[h, role, n], es.at[h, role, n], er.at[h, role, n],
                    peer(h, role_step(h, 1 - role)),
                )
                c.start()
                trades[h, role, n] = c

    def place(h, slot):
        return pl.ds(pl.multiple_of(slot * 128, 128), 128)

    for h in both:
        for role in both:
            for o in both:
                part = term(h, role, 0, pos[h], o)
                wide[h, place(h, 2 * role + o), :] = part[:, 0:128]
                wide[2 + h, place(h, 2 * role + o), :] = part[:, 128:256]
    for h in both:
        wide2[pl.ds(h, T, stride=2), :] = jnp.transpose(dqf[h].astype(F32))
    qg_ref[...] = wide2[0 : 2 * T, :].astype(BF16)
    ends = [dk[h].end() for h in both]
    for p, ref in ((0, kg_ref), (1, vg_ref)):
        for h in both:
            wide2[pl.ds(2 * T * p + h, T, stride=2), :] = ends[h][p]
        ref[...] = wide2[2 * T * p : 2 * T * p + 2 * T, :].astype(BF16)
    for n in both:
        for h in both:
            o = odd[h] if n == 0 else 1 - odd[h]
            for role in both:
                trades[h, role, n].wait_recv()
                got = erx[h, role, n].astype(F32)
                wide[h, place(h, 2 * role + o), :] += got[:, 0:128]
                wide[2 + h, place(h, 2 * role + o), :] += got[:, 128:256]
            if n == 0:
                wb[h].far()
            else:
                wb[h].direct()
    for h in both:
        wg_ref[:, h * W : h * W + W] = jnp.transpose(wb[h].end())

    for c in first.values():
        c.wait_send()
    for c in second:
        c.wait_send()
    for forward in (False, True):
        z_each(names, forward, wait_send)
    for c in shares + swaps + list(hands.values()) + list(trades.values()):
        c.wait_send()
    for group in (dq, dk, wb):
        for r in group:
            r.drain()


def put_kernel(*refs):
    sems = refs[8]
    copies = [pltpu.make_async_copy(refs[n], refs[4 + n], sems.at[n]) for n in range(4)]
    for c in copies:
        c.start()
    for c in copies:
        c.wait()


def body(latents, query_heads, key_heads, value_heads, map_outputs, log_sums, out_grad, mix_lambda, norm_gain):
    rows = 2 * T
    hbm = pl.BlockSpec(memory_space=pltpu.HBM)
    vmem = pl.BlockSpec(memory_space=pltpu.VMEM)
    out_shape = (
        jax.ShapeDtypeStruct((rows, W), BF16),
        jax.ShapeDtypeStruct((rows, W), BF16),
        jax.ShapeDtypeStruct((rows, W), BF16),
        jax.ShapeDtypeStruct((T, 2 * W), F32),
    )
    outs = pl.pallas_call(
        kernel,
        out_shape=tuple(pltpu.VMEM(o.shape, o.dtype) for o in out_shape),
        in_specs=[hbm] * 9,
        out_specs=(vmem, vmem, vmem, vmem),
        scratch_shapes=[
            pltpu.VMEM((rows, W), BF16),
            pltpu.VMEM((rows, W), BF16),
            pltpu.VMEM((rows, W), BF16),
            pltpu.VMEM((2 * rows, W), BF16),
            pltpu.VMEM((2, 2, T), F32),
            pltpu.VMEM((rows, W), BF16),
            pltpu.SMEM((2,), F32),
            pltpu.VMEM((1, W), F32),
            pltpu.VMEM((4, 4, T, T), BF16),
            pltpu.VMEM((2, 2, 2, 2, T, T), BF16),
            pltpu.VMEM((2, 4, 2, T, W), BF16),
            pltpu.VMEM((2, 4, 2, T, W), BF16),
            pltpu.VMEM((2, 4, 8, T), F32),
            pltpu.VMEM((2, 4, W, T), F32),
            pltpu.VMEM((2, 4, 2, T, W), F32),
            pltpu.VMEM((3, T, T), BF16),
            pltpu.VMEM((4, rows, W), F32),
            pltpu.VMEM((4 * T, W), F32),
            pltpu.VMEM((2, W, T), BF16),
            pltpu.VMEM((2, 2, W, T), BF16),
            pltpu.VMEM((2, 3, W, T), BF16),
            pltpu.VMEM((2, 3, W, T), BF16),
            pltpu.VMEM((2, 6, T, W), BF16),
            pltpu.VMEM((2, 6, T, W), BF16),
            pltpu.VMEM((2, 2, 2, W, T), BF16),
            pltpu.VMEM((2, 2, 2, W, T), BF16),
            pltpu.VMEM((2, 3, W, T), BF16),
            pltpu.VMEM((2, 3, W, T), BF16),
            pltpu.VMEM((2, 2, 2, W, T), F32),
            pltpu.SemaphoreType.DMA((24,)),
            pltpu.SemaphoreType.DMA((2, 2, 10)),
            pltpu.SemaphoreType.DMA((2, 2, 10)),
            pltpu.SemaphoreType.DMA((2, 24)),
            pltpu.SemaphoreType.DMA((2, 24)),
            pltpu.SemaphoreType.DMA((2, 2, 2)),
            pltpu.SemaphoreType.DMA((2, 2, 2)),
            pltpu.SemaphoreType.DMA((2, 2)),
            pltpu.SemaphoreType.DMA((2, 2)),
            pltpu.SemaphoreType.DMA((2, 2)),
            pltpu.SemaphoreType.DMA((2, 2)),
            pltpu.SemaphoreType.DMA((2, 2, 2)),
            pltpu.SemaphoreType.DMA((2, 2, 2)),
        ],
        compiler_params=pltpu.CompilerParams(
            collective_id=0, has_side_effects=True, vmem_limit_bytes=VMEM_ALL
        ),
    )(
        query_heads.reshape(rows, W),
        key_heads.reshape(rows, W),
        value_heads.reshape(rows, W),
        map_outputs.reshape(2 * rows, W),
        jnp.transpose(log_sums, (1, 2, 0)),
        out_grad.reshape(rows, W),
        mix_lambda,
        norm_gain.reshape(1, W),
        latents,
    )
    qg, kg, vg, wg = pl.pallas_call(
        put_kernel,
        out_shape=out_shape,
        in_specs=[vmem] * 4,
        out_specs=(hbm, hbm, hbm, hbm),
        scratch_shapes=[pltpu.SemaphoreType.DMA((4,))],
        compiler_params=pltpu.CompilerParams(vmem_limit_bytes=1024 * 1024),
    )(*outs)
    shape = query_heads.shape
    return (qg.reshape(shape), kg.reshape(shape), vg.reshape(shape), wg)


def solution(mesh):
    placed = (
        P("sp", None),
        P("sp", "tp", None),
        P("sp", "tp", None),
        P("sp", "tp", None),
        P("sp", None, "tp", None),
        P("sp", "tp", None),
        P("sp", "tp", None),
        P("tp"),
        P(),
    )
    return jax.shard_map(
        body,
        mesh=mesh,
        in_specs=placed,
        out_specs=(P("sp", "tp", None), P("sp", "tp", None), P("sp", "tp", None), P("sp", "tp")),
        check_vma=False,
    )
```

```python
import functools

import jax
import jax.numpy as jnp
from jax import lax
from jax.experimental import pallas as pl
from jax.experimental.pallas import tpu as pltpu
from jax.sharding import PartitionSpec as P

F32 = jnp.float32
BF16 = jnp.bfloat16
EPSILON = 1e-05
LOG2E = 1.4426950408889634
SCALE = 0.125
T = 256
W = 128
VMEM_ALL = 66200000
NT = (((1,), (1,)), ((), ()))


def dot(a, b):
    return jnp.dot(a, b, preferred_element_type=F32)


def dot_nt(a, b):
    return lax.dot_general(a, b, NT, preferred_element_type=F32)


def kernel(
    q_hbm, k_hbm, v_hbm, mo_hbm, lse_hbm, og_hbm, lam_hbm, gain_hbm, lat_hbm,
    qg_ref, kg_ref, vg_ref, wg_ref,
    q_in, k_in, v_in, mo_in, lse_in, og_in, lam_in, gain_in,
    lat, lx, qdo, kv, st, dqt, dkv, wds, wide, wide2, dqf, dqg,
    qtx, qrx, ktx, krx, etx, erx, btx, brx, pre,
    in_sem, gs, gr, rs, rr, ls, lr, ds, dr, hs, hr, es, er,
):
    sp = lax.axis_index("sp")
    tp = lax.axis_index("tp")
    z = sp // 4
    y = sp % 4
    pos = (y, z)

    def ring(axis, step):
        return lax.rem(pos[axis] + step + 4, 4)

    def peer(axis, step):
        moved = ring(axis, step)
        return (z * 4 + moved if axis == 0 else moved * 4 + y, tp)

    def remote(src, dst, send, recv, device):
        return pltpu.make_async_remote_copy(
            src_ref=src, dst_ref=dst, send_sem=send, recv_sem=recv,
            device_id=device, device_id_type=pl.DeviceIdType.MESH,
        )

    def role_step(axis, role):
        sign = 1 - 2 * (pos[axis] % 2)
        return sign if role == 0 else -sign

    core = tp % 2
    sibling = (sp, tp + 1 - 2 * core)
    barrier = pltpu.get_barrier_semaphore()
    pl.semaphore_signal(barrier, inc=1, device_id=sibling, device_id_type=pl.DeviceIdType.MESH)
    for axis in (0, 1):
        for step in (1, -1, 2):
            pl.semaphore_signal(
                barrier, inc=1, device_id=peer(axis, step), device_id_type=pl.DeviceIdType.MESH
            )
    sources = (q_hbm, k_hbm, v_hbm, og_hbm, mo_hbm, lse_hbm, lam_hbm, gain_hbm)
    targets = (q_in, k_in, v_in, og_in, mo_in, lse_in, lam_in, gain_in)
    loads = [pltpu.make_async_copy(a, b, in_sem.at[n]) for n, (a, b) in enumerate(zip(sources, targets))]
    loads += [
        pltpu.make_async_copy(lat_hbm.at[:, n * T : n * T + T], lat.at[n // 4, n % 4], in_sem.at[8 + n])
        for n in range(16)
    ]
    for c in loads:
        c.start()

    qpos = (y, z)
    kpos = (z, y)
    qh = (0, 1)
    kh = (1, 0)
    first = {}

    def item(axis, name, slot):
        if name == "q":
            return qdo.at[qh[axis], slot, 0]
        if name == "do":
            return qdo.at[qh[axis], slot, 1]
        if name == "st":
            return st.at[qh[axis], slot]
        if name == "k":
            return kv.at[kh[axis], slot, 0]
        return kv.at[kh[axis], slot, 1]

    names = ("q", "k", "v", "do", "st")

    def gather_copy(axis, d, name, slot, forward):
        n = names.index(name) + (5 if forward else 0)
        ref = item(axis, name, slot)
        step = 1 if d == 0 else -1
        return remote(ref, ref, gs.at[axis, d, n], gr.at[axis, d, n], peer(axis, step))

    ups = ("k", "v")
    downs = ("q", "do", "st")

    def z_each(some, forward, do_it):
        if forward:
            middle = (z == 1) | (z == 2)
            cases = ((0, middle, ups, -1), (1, middle, downs, 1))
        else:
            cases = ((0, z < 3, ups, 0), (0, z == 3, downs, 0), (1, z > 0, downs, 0), (1, z == 0, ups, 0))
        for d, wanted, group, shift in cases:
            mine = [name for name in some if name in group]
            if mine:
                @pl.when(wanted)
                def _():
                    for name in mine:
                        do_it(gather_copy(1, d, name, ring(1, shift), forward))

    def z_arrived(some, forward):
        if forward:
            cases = ((0, z >= 2, ups, 2), (1, z < 2, downs, 2))
        else:
            cases = ((0, z > 0, ups, -1), (0, z == 0, downs, -1), (1, z < 3, downs, 1), (1, z == 3, ups, 1))
        for d, wanted, group, shift in cases:
            mine = [name for name in some if name in group]
            if mine:
                @pl.when(wanted)
                def _():
                    for name in mine:
                        gather_copy(1, d, name, ring(1, shift), forward).wait_recv()

    def start(c):
        c.start()

    def wait_send(c):
        c.wait_send()

    def send_own(some):
        for name in some:
            for d in (0, 1):
                c = gather_copy(0, d, name, y, False)
                c.start()
                first[d, name] = c
            z_each((name,), False, start)

    for n, (name, ref) in enumerate((("q", q_in), ("k", k_in), ("v", v_in))):
        loads[n].wait()
        wide[n] = ref[...].astype(F32)
        for h in (0, 1):
            part = wide[n, pl.ds(h, T, stride=2), :].astype(BF16)
            if n == 0:
                qdo[h, qpos[h], 0] = part
            else:
                kv[h, kpos[h], n - 1] = part
        if n == 0:
            pl.semaphore_wait(barrier, 7)
        send_own((name,))

    for c in loads[3:8]:
        c.wait()
    wide[3] = og_in[...].astype(F32)
    wide2[...] = mo_in[...].astype(F32)
    gain = gain_in[...]
    for h in (0, 1):
        lam = lam_in[h]
        m1 = wide2[pl.ds(h, T, stride=4), :]
        m2 = wide2[pl.ds(2 + h, T, stride=4), :]
        comb = m1 - lam * m2
        inv = lax.rsqrt(jnp.mean(comb * comb, axis=-1, keepdims=True) + EPSILON)
        wtd = gain * wide[3, pl.ds(h, T, stride=2), :]
        cross = jnp.mean(comb * wtd, axis=-1, keepdims=True)
        grad = (inv * wtd - inv * inv * inv * comb * cross).astype(BF16)
        qdo[h, qpos[h], 1] = grad
        gf = grad.astype(F32)
        r1 = jnp.sum(jnp.transpose(gf * m1), axis=0, keepdims=True)
        r2 = jnp.sum(jnp.transpose(gf * m2), axis=0, keepdims=True)
        lam_row = jnp.full((1, T), lam, F32)
        st[h, qpos[h], 0:1] = lse_in[h, 0:1, :] * LOG2E
        st[h, qpos[h], 1:2] = (lse_in[h, 1:2, :] - jnp.log(lam_row)) * LOG2E
        st[h, qpos[h], 2:3] = r1
        st[h, qpos[h], 3:4] = r2
        st[h, qpos[h], 4:8] = jnp.zeros((4, T), F32)
    send_own(("do", "st"))

    dqt[...] = jnp.zeros_like(dqt)
    dkv[...] = jnp.zeros_like(dkv)

    lane = lax.broadcasted_iota(jnp.int32, (T, W), 1)

    def split_queries(h, qs):
        q = qdo[h, qs, 0]
        zero = jnp.zeros_like(q)
        return jnp.where(lane < 64, q, zero), jnp.where(lane < 64, zero, -q)

    def scores(h, qs, ks, masked):
        q1, q2 = split_queries(h, qs)
        do = qdo[h, qs, 1]
        half = T // 2
        for c in (0, half):
            k = kv[h, ks, 0, c : c + half]
            v = kv[h, ks, 1, c : c + half]
            s1 = dot_nt(k, q1)
            s2 = dot_nt(k, q2)
            dp = dot_nt(v, do)
            p1 = jnp.exp2(s1 * (SCALE * LOG2E) - st[h, qs, 0:1])
            p2 = jnp.exp2(s2 * (-SCALE * LOG2E) - st[h, qs, 1:2])
            if masked:
                rows = lax.broadcasted_iota(jnp.int32, (half, T), 0) + c
                cols = lax.broadcasted_iota(jnp.int32, (half, T), 1)
                keep = rows <= cols
                p1 = jnp.where(keep, p1, 0.0)
                p2 = jnp.where(keep, p2, 0.0)
            wds[0, c : c + half] = (p1 - p2).astype(BF16)
            wds[1, c : c + half] = (p1 * (dp - st[h, qs, 2:3])).astype(BF16)
            wds[2, c : c + half] = (p2 * (dp - st[h, qs, 3:4])).astype(BF16)

    def products(h, qs, ks):
        q1, q2 = split_queries(h, qs)
        w, d1, d2 = wds[0], wds[1], wds[2]
        kt = jnp.transpose(kv[h, ks, 0])
        dqt[h, qs, 0:64] += dot(kt[0:64], d1)
        dqt[h, qs, 64:128] -= dot(kt[64:128], d2)
        dkv[h, ks, 0] += dot(d1, q1) + dot(d2, q2)
        dkv[h, ks, 1] += dot(w, qdo[h, qs, 1])

    def maybe_unit(h, i, j, before):
        qo = jnp.where(i < 2, i, 5 - i)
        ko = jnp.where(j < 2, j, 5 - j)
        qbase = jnp.where(h == 0, y, z)
        kbase = jnp.where(h == 0, z, y)
        qs = (qbase + qo) % 4
        ks = (kbase + ko) % 4
        q_block = jnp.where(h == 0, z * 4 + qs, qs * 4 + y)
        k_block = jnp.where(h == 0, ks * 4 + y, z * 4 + ks)
        wanted = k_block < q_block

        @pl.when(wanted)
        def _():
            products(*before)
            scores(h, qs, ks, False)

        return tuple(jnp.where(wanted, a, b) for a, b in zip((h, qs, ks), before))

    def some_units(count, which, before, fresh):
        if fresh:
            wds[...] = jnp.zeros_like(wds)

        def step(n, carry):
            return maybe_unit(*which(n), carry)

        return lax.fori_loop(0, count, step, before)

    scores(0, y, z, True)
    products(0, y, z)
    scores(1, z, y, True)
    pending = (jnp.int32(1), z, y)

    second = []
    rows = pl.ds(pl.multiple_of(core * 128, 128), 128)
    shares = []

    def share(axis):
        for role in (0, 1):
            step = role_step(axis, role)
            for w, owner in enumerate((ring(axis, step), ring(axis, 2))):
                some = slice(2 * role, 2 * role + 2)
                src = lat.at[some, owner, rows, :] if axis == 0 else lat.at[owner, some, rows, :]
                c = remote(
                    src, lx.at[axis, role, w, :, rows, :], ls.at[axis, role, w], lr.at[axis, role, w],
                    peer(axis, step),
                )
                c.start()
                shares.append(c)

    def pass_on(some):
        for name in some:
            for d in (0, 1):
                first[d, name].wait_recv()
                if d == (0 if name in ("q", "k") else 1):
                    c = gather_copy(0, d, name, ring(0, -1 if d == 0 else 1), True)
                    c.start()
                    second.append(c)

    pass_on(("q", "k"))
    for some in (("q", "k"), ("v",), ("do", "st")):
        z_arrived(some, False)
        z_each(some, True, start)
    for c in loads[8:]:
        c.wait()
    share(1)
    pending = some_units(
        4, lambda n: (n // 2, jnp.where(n < 2, 0, n - 1), jnp.where(n < 2, n + 1, 0)), pending, False
    )
    pass_on(("v", "do", "st"))

    share(0)

    pending = some_units(
        12,
        lambda n: (
            n // 6,
            jnp.where(n < 6, n // 3 + 1, n % 3),
            jnp.where(n < 6, n % 3, (n - 6) // 3 + 1),
        ),
        pending,
        False,
    )
    z_arrived(names, True)
    pending = some_units(
        6, lambda n: (n // 3, jnp.where(n < 3, n, 3), jnp.where(n < 3, 3, n - 3)), pending, False
    )
    for c in second:
        c.wait_recv()

    class Reduction:
        def __init__(self, tx, rx, axis, base, get):
            self.tx, self.rx, self.axis, self.base, self.get = tx, rx, axis, base, get
            self.out = {}

        def go(self, j, value, step):
            axis = self.axis
            self.tx[axis, j] = value.astype(BF16)
            c = remote(
                self.tx.at[axis, j], self.rx.at[axis, j],
                rs.at[axis, self.base + j], rr.at[axis, self.base + j], peer(axis, step),
            )
            c.start()
            self.out[j] = c

        def far(self):
            slot = ring(self.axis, 2)
            self.go(0, self.get(slot, 0), 1)
            self.go(1, self.get(slot, 1), -1)

        def direct(self):
            self.go(2, self.get(ring(self.axis, 1), 1), 1)
            self.go(3, self.get(ring(self.axis, -1), 0), -1)

        def summed(self):
            for j, step in ((0, 1), (1, -1)):
                mine = self.get(ring(self.axis, step), j)
                self.out[j].wait_recv()
                self.go(4 + j, mine + self.rx[self.axis, j].astype(F32), step)

        def end(self):
            own0 = self.get(pos[self.axis], 0)
            own1 = self.get(pos[self.axis], 1)
            for j in (2, 3, 4, 5):
                self.out[j].wait_recv()
            rx = self.rx
            r0 = own0 + rx[self.axis, 3].astype(F32) + rx[self.axis, 4].astype(F32)
            r1 = own1 + rx[self.axis, 2].astype(F32) + rx[self.axis, 5].astype(F32)
            return r0, r1

        def drain(self):
            for c in self.out.values():
                c.wait_send()

    class Direct:
        def __init__(self, tx, rx, axis, base, get):
            self.tx, self.rx, self.axis, self.base, self.get = tx, rx, axis, base, get
            self.out = {}

        def go(self, j, step):
            axis = self.axis
            self.tx[axis, j] = self.get(ring(axis, step)).astype(BF16)
            c = remote(
                self.tx.at[axis, j], self.rx.at[axis, j],
                rs.at[axis, self.base + j], rr.at[axis, self.base + j], peer(axis, step),
            )
            c.start()
            self.out[j] = c

        def far(self):
            self.go(0, 2)

        def direct(self):
            self.go(1, 1)
            self.go(2, -1)

        def end(self):
            total = self.get(pos[self.axis])
            for j in (1, 2, 0):
                self.out[j].wait_recv()
                total = total + self.rx[self.axis, j].astype(F32)
            return total

        def drain(self):
            for c in self.out.values():
                c.wait_send()

    def get_dq(h):
        return lambda slot: dqt[h, slot] * SCALE

    def get_dkv(h):
        return lambda slot, p: dkv[h, slot, p] * (SCALE if p == 0 else 1.0)

    def get_last(h):
        def get(slot):
            rows = pl.ds(pl.multiple_of(slot * 128, 128), 128)
            return jnp.concatenate([wide[h, rows, :], wide[2 + h, rows, :]], axis=1)

        return get

    both = (0, 1)
    dq = [Direct(qtx, qrx, h, 0, get_dq(h)) for h in both]
    dk = [Reduction(ktx, krx, 1 - h, 18, get_dkv(h)) for h in both]
    wb = [Direct(btx, brx, 1 - h, 12, get_last(h)) for h in both]

    pending = some_units(
        5, lambda n: (jnp.where(n == 0, 1, 0), jnp.int32(3), jnp.where(n == 0, 3, n - 1)), pending, False
    )
    products(*pending)
    for h in both:
        dq[h].far()
    dq[0].direct()
    pending = some_units(3, lambda n: (jnp.int32(1), n, jnp.int32(3)), pending, True)
    products(*pending)
    dq[1].direct()
    for h in both:
        dk[h].direct()
    swaps = []
    for c in shares:
        c.wait_recv()
    for axis in (0, 1):
        for role in (0, 1):
            ref = lx.at[axis, role, :, :, rows, :]
            c = remote(ref, ref, ds.at[axis, role], dr.at[axis, role], sibling)
            c.start()
            swaps.append(c)
    def block(h, owner, o):
        return lat[o, owner] if h == 0 else lat[owner, o]

    def term(h, role, w, owner, o):
        near = dot(dqf[h], block(h, owner, 2 * role + o))
        return near + dot(dqg[h, role], lx[h, role, w, o])

    hands = {}
    for h in both:
        dqf[h] = dq[h].end().astype(BF16)
        for role in both:
            c = remote(
                dqf.at[h], dqg.at[h, role], hs.at[h, role], hr.at[h, role], peer(h, role_step(h, role))
            )
            c.start()
            hands[h, role] = c
    for h in both:
        dk[h].far()
    odd = [pos[1 - h] % 2 for h in both]
    trades = {}
    for h in both:
        for role in both:
            for n, o in enumerate((odd[h], 1 - odd[h])):
                pre[h, role, n] = dot(dqf[h], block(h, ring(h, role_step(h, 1 - role)), 2 * role + o))
    for c in swaps:
        c.wait_recv()
    for n in both:
        for h in both:
            o = odd[h] if n == 0 else 1 - odd[h]
            for role in both:
                if n == 0:
                    hands[h, role].wait_recv()
                etx[h, role, n] = (pre[h, role, n] + dot(dqg[h, role], lx[h, role, 1, o])).astype(BF16)
                c = remote(
                    etx.at[h, role, n], erx.at[h, role, n], es.at[h, role, n], er.at[h, role, n],
                    peer(h, role_step(h, 1 - role)),
                )
                c.start()
                trades[h, role, n] = c

    for h in both:
        dk[h].summed()

    def place(h, slot):
        return pl.ds(pl.multiple_of(slot * 128, 128), 128)

    for h in both:
        for role in both:
            for o in both:
                part = term(h, role, 0, pos[h], o)
                wide[h, place(h, 2 * role + o), :] = part[:, 0:128]
                wide[2 + h, place(h, 2 * role + o), :] = part[:, 128:256]
    for h in both:
        wide2[pl.ds(h, T, stride=2), :] = jnp.transpose(dqf[h].astype(F32))
    qg_ref[...] = wide2[0 : 2 * T, :].astype(BF16)
    for n in both:
        for h in both:
            o = odd[h] if n == 0 else 1 - odd[h]
            for role in both:
                trades[h, role, n].wait_recv()
                got = erx[h, role, n].astype(F32)
                wide[h, place(h, 2 * role + o), :] += got[:, 0:128]
                wide[2 + h, place(h, 2 * role + o), :] += got[:, 128:256]
            if n == 0:
                wb[h].far()
            else:
                wb[h].direct()
    ends = [dk[h].end() for h in both]
    for p, ref in ((0, kg_ref), (1, vg_ref)):
        for h in both:
            wide2[pl.ds(2 * T * p + h, T, stride=2), :] = ends[h][p]
        ref[...] = wide2[2 * T * p : 2 * T * p + 2 * T, :].astype(BF16)
    for h in both:
        wg_ref[:, h * W : h * W + W] = jnp.transpose(wb[h].end())

    for c in first.values():
        c.wait_send()
    for c in second:
        c.wait_send()
    for forward in (False, True):
        z_each(names, forward, wait_send)
    for c in shares + swaps + list(hands.values()) + list(trades.values()):
        c.wait_send()
    for group in (dq, dk, wb):
        for r in group:
            r.drain()


def put_kernel(*refs):
    sems = refs[8]
    copies = [pltpu.make_async_copy(refs[n], refs[4 + n], sems.at[n]) for n in range(4)]
    for c in copies:
        c.start()
    for c in copies:
        c.wait()


def body(latents, query_heads, key_heads, value_heads, map_outputs, log_sums, out_grad, mix_lambda, norm_gain):
    rows = 2 * T
    hbm = pl.BlockSpec(memory_space=pltpu.HBM)
    vmem = pl.BlockSpec(memory_space=pltpu.VMEM)
    out_shape = (
        jax.ShapeDtypeStruct((rows, W), BF16),
        jax.ShapeDtypeStruct((rows, W), BF16),
        jax.ShapeDtypeStruct((rows, W), BF16),
        jax.ShapeDtypeStruct((T, 2 * W), F32),
    )
    outs = pl.pallas_call(
        kernel,
        out_shape=tuple(pltpu.VMEM(o.shape, o.dtype) for o in out_shape),
        in_specs=[hbm] * 9,
        out_specs=(vmem, vmem, vmem, vmem),
        scratch_shapes=[
            pltpu.VMEM((rows, W), BF16),
            pltpu.VMEM((rows, W), BF16),
            pltpu.VMEM((rows, W), BF16),
            pltpu.VMEM((2 * rows, W), BF16),
            pltpu.VMEM((2, 2, T), F32),
            pltpu.VMEM((rows, W), BF16),
            pltpu.SMEM((2,), F32),
            pltpu.VMEM((1, W), F32),
            pltpu.VMEM((4, 4, T, T), BF16),
            pltpu.VMEM((2, 2, 2, 2, T, T), BF16),
            pltpu.VMEM((2, 4, 2, T, W), BF16),
            pltpu.VMEM((2, 4, 2, T, W), BF16),
            pltpu.VMEM((2, 4, 8, T), F32),
            pltpu.VMEM((2, 4, W, T), F32),
            pltpu.VMEM((2, 4, 2, T, W), F32),
            pltpu.VMEM((3, T, T), BF16),
            pltpu.VMEM((4, rows, W), F32),
            pltpu.VMEM((4 * T, W), F32),
            pltpu.VMEM((2, W, T), BF16),
            pltpu.VMEM((2, 2, W, T), BF16),
            pltpu.VMEM((2, 3, W, T), BF16),
            pltpu.VMEM((2, 3, W, T), BF16),
            pltpu.VMEM((2, 6, T, W), BF16),
            pltpu.VMEM((2, 6, T, W), BF16),
            pltpu.VMEM((2, 2, 2, W, T), BF16),
            pltpu.VMEM((2, 2, 2, W, T), BF16),
            pltpu.VMEM((2, 3, W, T), BF16),
            pltpu.VMEM((2, 3, W, T), BF16),
            pltpu.VMEM((2, 2, 2, W, T), F32),
            pltpu.SemaphoreType.DMA((24,)),
            pltpu.SemaphoreType.DMA((2, 2, 10)),
            pltpu.SemaphoreType.DMA((2, 2, 10)),
            pltpu.SemaphoreType.DMA((2, 24)),
            pltpu.SemaphoreType.DMA((2, 24)),
            pltpu.SemaphoreType.DMA((2, 2, 2)),
            pltpu.SemaphoreType.DMA((2, 2, 2)),
            pltpu.SemaphoreType.DMA((2, 2)),
            pltpu.SemaphoreType.DMA((2, 2)),
            pltpu.SemaphoreType.DMA((2, 2)),
            pltpu.SemaphoreType.DMA((2, 2)),
            pltpu.SemaphoreType.DMA((2, 2, 2)),
            pltpu.SemaphoreType.DMA((2, 2, 2)),
        ],
        compiler_params=pltpu.CompilerParams(
            collective_id=0, has_side_effects=True, vmem_limit_bytes=VMEM_ALL
        ),
    )(
        query_heads.reshape(rows, W),
        key_heads.reshape(rows, W),
        value_heads.reshape(rows, W),
        map_outputs.reshape(2 * rows, W),
        jnp.transpose(log_sums, (1, 2, 0)),
        out_grad.reshape(rows, W),
        mix_lambda,
        norm_gain.reshape(1, W),
        latents,
    )
    qg, kg, vg, wg = pl.pallas_call(
        put_kernel,
        out_shape=out_shape,
        in_specs=[vmem] * 4,
        out_specs=(hbm, hbm, hbm, hbm),
        scratch_shapes=[pltpu.SemaphoreType.DMA((4,))],
        compiler_params=pltpu.CompilerParams(vmem_limit_bytes=1024 * 1024),
    )(*outs)
    shape = query_heads.shape
    return (qg.reshape(shape), kg.reshape(shape), vg.reshape(shape), wg)


def solution(mesh):
    placed = (
        P("sp", None),
        P("sp", "tp", None),
        P("sp", "tp", None),
        P("sp", "tp", None),
        P("sp", None, "tp", None),
        P("sp", "tp", None),
        P("sp", "tp", None),
        P("tp"),
        P(),
    )
    return jax.shard_map(
        body,
        mesh=mesh,
        in_specs=placed,
        out_specs=(P("sp", "tp", None), P("sp", "tp", None), P("sp", "tp", None), P("sp", "tp")),
        check_vma=False,
    )
```

```python
import functools

import jax
import jax.numpy as jnp
from jax import lax
from jax.experimental import pallas as pl
from jax.experimental.pallas import tpu as pltpu
from jax.sharding import PartitionSpec as P

F32 = jnp.float32
BF16 = jnp.bfloat16
EPSILON = 1e-05
LOG2E = 1.4426950408889634
SCALE = 0.125
T = 256
W = 128
VMEM_ALL = 66200000
NT = (((1,), (1,)), ((), ()))


def dot(a, b):
    return jnp.dot(a, b, preferred_element_type=F32)


def dot_nt(a, b):
    return lax.dot_general(a, b, NT, preferred_element_type=F32)


def kernel(
    q_hbm, k_hbm, v_hbm, mo_hbm, lse_hbm, og_hbm, lam_hbm, gain_hbm, lat_hbm,
    qg_ref, kg_ref, vg_ref, wg_ref,
    q_in, k_in, v_in, mo_in, lse_in, og_in, lam_in, gain_in,
    lat, lx, qdo, kv, st, dqt, dkv, wds, wide, wide2, dqf, dqg,
    qtx, qrx, ktx, krx, etx, erx, btx, brx, pre,
    in_sem, gs, gr, rs, rr, ls, lr, ds, dr, hs, hr, es, er,
):
    sp = lax.axis_index("sp")
    tp = lax.axis_index("tp")
    z = sp // 4
    y = sp % 4
    pos = (y, z)

    def ring(axis, step):
        return lax.rem(pos[axis] + step + 4, 4)

    def peer(axis, step):
        moved = ring(axis, step)
        return (z * 4 + moved if axis == 0 else moved * 4 + y, tp)

    def remote(src, dst, send, recv, device):
        return pltpu.make_async_remote_copy(
            src_ref=src, dst_ref=dst, send_sem=send, recv_sem=recv,
            device_id=device, device_id_type=pl.DeviceIdType.MESH,
        )

    def role_step(axis, role):
        sign = 1 - 2 * (pos[axis] % 2)
        return sign if role == 0 else -sign

    core = tp % 2
    sibling = (sp, tp + 1 - 2 * core)
    barrier = pltpu.get_barrier_semaphore()
    pl.semaphore_signal(barrier, inc=1, device_id=sibling, device_id_type=pl.DeviceIdType.MESH)
    for axis in (0, 1):
        for step in (1, -1, 2):
            pl.semaphore_signal(
                barrier, inc=1, device_id=peer(axis, step), device_id_type=pl.DeviceIdType.MESH
            )
    sources = (q_hbm, k_hbm, v_hbm, og_hbm, mo_hbm, lse_hbm, lam_hbm, gain_hbm)
    targets = (q_in, k_in, v_in, og_in, mo_in, lse_in, lam_in, gain_in)
    loads = [pltpu.make_async_copy(a, b, in_sem.at[n]) for n, (a, b) in enumerate(zip(sources, targets))]
    loads += [
        pltpu.make_async_copy(lat_hbm.at[:, n * T : n * T + T], lat.at[n // 4, n % 4], in_sem.at[8 + n])
        for n in range(16)
    ]
    for c in loads:
        c.start()

    qpos = (y, z)
    kpos = (z, y)
    qh = (0, 1)
    kh = (1, 0)
    first = {}

    def item(axis, name, slot):
        if name == "q":
            return qdo.at[qh[axis], slot, 0]
        if name == "do":
            return qdo.at[qh[axis], slot, 1]
        if name == "st":
            return st.at[qh[axis], slot]
        if name == "k":
            return kv.at[kh[axis], slot, 0]
        return kv.at[kh[axis], slot, 1]

    names = ("q", "k", "v", "do", "st")

    def gather_copy(axis, d, name, slot, forward):
        n = names.index(name) + (5 if forward else 0)
        ref = item(axis, name, slot)
        step = 1 if d == 0 else -1
        return remote(ref, ref, gs.at[axis, d, n], gr.at[axis, d, n], peer(axis, step))

    ups = ("k", "v")
    downs = ("q", "do", "st")

    def z_each(some, forward, do_it):
        if forward:
            middle = (z == 1) | (z == 2)
            cases = ((0, middle, ups, -1), (1, middle, downs, 1))
        else:
            cases = ((0, z < 3, ups, 0), (0, z == 3, downs, 0), (1, z > 0, downs, 0), (1, z == 0, ups, 0))
        for d, wanted, group, shift in cases:
            mine = [name for name in some if name in group]
            if mine:
                @pl.when(wanted)
                def _():
                    for name in mine:
                        do_it(gather_copy(1, d, name, ring(1, shift), forward))

    def z_arrived(some, forward):
        if forward:
            cases = ((0, z >= 2, ups, 2), (1, z < 2, downs, 2))
        else:
            cases = ((0, z > 0, ups, -1), (0, z == 0, downs, -1), (1, z < 3, downs, 1), (1, z == 3, ups, 1))
        for d, wanted, group, shift in cases:
            mine = [name for name in some if name in group]
            if mine:
                @pl.when(wanted)
                def _():
                    for name in mine:
                        gather_copy(1, d, name, ring(1, shift), forward).wait_recv()

    def start(c):
        c.start()

    def wait_send(c):
        c.wait_send()

    def send_own(some):
        for name in some:
            for d in (0, 1):
                c = gather_copy(0, d, name, y, False)
                c.start()
                first[d, name] = c
            z_each((name,), False, start)

    for n, (name, ref) in enumerate((("q", q_in), ("k", k_in), ("v", v_in))):
        loads[n].wait()
        wide[n] = ref[...].astype(F32)
        for h in (0, 1):
            part = wide[n, pl.ds(h, T, stride=2), :].astype(BF16)
            if n == 0:
                qdo[h, qpos[h], 0] = part
            else:
                kv[h, kpos[h], n - 1] = part
        if n == 0:
            pl.semaphore_wait(barrier, 7)
        send_own((name,))

    for c in loads[3:8]:
        c.wait()
    wide[3] = og_in[...].astype(F32)
    wide2[...] = mo_in[...].astype(F32)
    gain = gain_in[...]
    for h in (0, 1):
        lam = lam_in[h]
        m1 = wide2[pl.ds(h, T, stride=4), :]
        m2 = wide2[pl.ds(2 + h, T, stride=4), :]
        comb = m1 - lam * m2
        inv = lax.rsqrt(jnp.mean(comb * comb, axis=-1, keepdims=True) + EPSILON)
        wtd = gain * wide[3, pl.ds(h, T, stride=2), :]
        cross = jnp.mean(comb * wtd, axis=-1, keepdims=True)
        grad = (inv * wtd - inv * inv * inv * comb * cross).astype(BF16)
        qdo[h, qpos[h], 1] = grad
        gf = grad.astype(F32)
        r1 = jnp.sum(jnp.transpose(gf * m1), axis=0, keepdims=True)
        r2 = jnp.sum(jnp.transpose(gf * m2), axis=0, keepdims=True)
        lam_row = jnp.full((1, T), lam, F32)
        st[h, qpos[h], 0:1] = lse_in[h, 0:1, :] * LOG2E
        st[h, qpos[h], 1:2] = (lse_in[h, 1:2, :] - jnp.log(lam_row)) * LOG2E
        st[h, qpos[h], 2:3] = r1
        st[h, qpos[h], 3:4] = r2
        st[h, qpos[h], 4:8] = jnp.zeros((4, T), F32)
    send_own(("do", "st"))

    dqt[...] = jnp.zeros_like(dqt)
    dkv[...] = jnp.zeros_like(dkv)

    lane = lax.broadcasted_iota(jnp.int32, (T, W), 1)

    def split_queries(h, qs):
        q = qdo[h, qs, 0]
        zero = jnp.zeros_like(q)
        return jnp.where(lane < 64, q, zero), jnp.where(lane < 64, zero, -q)

    def scores(h, qs, ks, masked):
        q1, q2 = split_queries(h, qs)
        do = qdo[h, qs, 1]
        half = T // 2
        for c in (0, half):
            k = kv[h, ks, 0, c : c + half]
            v = kv[h, ks, 1, c : c + half]
            s1 = dot_nt(k, q1)
            s2 = dot_nt(k, q2)
            dp = dot_nt(v, do)
            p1 = jnp.exp2(s1 * (SCALE * LOG2E) - st[h, qs, 0:1])
            p2 = jnp.exp2(s2 * (-SCALE * LOG2E) - st[h, qs, 1:2])
            if masked:
                rows = lax.broadcasted_iota(jnp.int32, (half, T), 0) + c
                cols = lax.broadcasted_iota(jnp.int32, (half, T), 1)
                keep = rows <= cols
                p1 = jnp.where(keep, p1, 0.0)
                p2 = jnp.where(keep, p2, 0.0)
            wds[0, c : c + half] = (p1 - p2).astype(BF16)
            wds[1, c : c + half] = (p1 * (dp - st[h, qs, 2:3])).astype(BF16)
            wds[2, c : c + half] = (p2 * (dp - st[h, qs, 3:4])).astype(BF16)

    def products(h, qs, ks):
        q1, q2 = split_queries(h, qs)
        w, d1, d2 = wds[0], wds[1], wds[2]
        kt = jnp.transpose(kv[h, ks, 0])
        dqt[h, qs, 0:64] += dot(kt[0:64], d1)
        dqt[h, qs, 64:128] -= dot(kt[64:128], d2)
        dkv[h, ks, 0] += dot(d1, q1) + dot(d2, q2)
        dkv[h, ks, 1] += dot(w, qdo[h, qs, 1])

    def maybe_unit(h, i, j, before):
        qo = jnp.where(i < 2, i, 5 - i)
        ko = jnp.where(j < 2, j, 5 - j)
        qbase = jnp.where(h == 0, y, z)
        kbase = jnp.where(h == 0, z, y)
        qs = (qbase + qo) % 4
        ks = (kbase + ko) % 4
        q_block = jnp.where(h == 0, z * 4 + qs, qs * 4 + y)
        k_block = jnp.where(h == 0, ks * 4 + y, z * 4 + ks)
        wanted = k_block < q_block

        @pl.when(wanted)
        def _():
            products(*before)
            scores(h, qs, ks, False)

        return tuple(jnp.where(wanted, a, b) for a, b in zip((h, qs, ks), before))

    def some_units(count, which, before, fresh):
        if fresh:
            wds[...] = jnp.zeros_like(wds)

        def step(n, carry):
            return maybe_unit(*which(n), carry)

        return lax.fori_loop(0, count, step, before)

    scores(0, y, z, True)
    products(0, y, z)
    scores(1, z, y, True)
    pending = (jnp.int32(1), z, y)

    second = []
    rows = pl.ds(pl.multiple_of(core * 128, 128), 128)
    shares = []

    def share(axis):
        for role in (0, 1):
            step = role_step(axis, role)
            for w, owner in enumerate((ring(axis, step), ring(axis, 2))):
                some = slice(2 * role, 2 * role + 2)
                src = lat.at[some, owner, rows, :] if axis == 0 else lat.at[owner, some, rows, :]
                c = remote(
                    src, lx.at[axis, role, w, :, rows, :], ls.at[axis, role, w], lr.at[axis, role, w],
                    peer(axis, step),
                )
                c.start()
                shares.append(c)

    def pass_on(some):
        for name in some:
            for d in (0, 1):
                first[d, name].wait_recv()
                if d == (0 if name in ("q", "k") else 1):
                    c = gather_copy(0, d, name, ring(0, -1 if d == 0 else 1), True)
                    c.start()
                    second.append(c)

    pass_on(("q", "k"))
    for some in (("q", "k"), ("v",), ("do", "st")):
        z_arrived(some, False)
        z_each(some, True, start)
    for c in loads[8:]:
        c.wait()
    share(1)
    pending = some_units(
        4, lambda n: (n // 2, jnp.where(n < 2, 0, n - 1), jnp.where(n < 2, n + 1, 0)), pending, False
    )
    pass_on(("v", "do", "st"))

    share(0)

    pending = some_units(
        12,
        lambda n: (
            n // 6,
            jnp.where(n < 6, n // 3 + 1, n % 3),
            jnp.where(n < 6, n % 3, (n - 6) // 3 + 1),
        ),
        pending,
        False,
    )
    z_arrived(names, True)
    pending = some_units(
        6, lambda n: (n // 3, jnp.where(n < 3, n, 3), jnp.where(n < 3, 3, n - 3)), pending, False
    )
    for c in second:
        c.wait_recv()

    class Reduction:
        def __init__(self, tx, rx, axis, base, get):
            self.tx, self.rx, self.axis, self.base, self.get = tx, rx, axis, base, get
            self.out = {}

        def go(self, j, value, step):
            axis = self.axis
            self.tx[axis, j] = value.astype(BF16)
            c = remote(
                self.tx.at[axis, j], self.rx.at[axis, j],
                rs.at[axis, self.base + j], rr.at[axis, self.base + j], peer(axis, step),
            )
            c.start()
            self.out[j] = c

        def far(self):
            slot = ring(self.axis, 2)
            self.go(0, self.get(slot, 0), 1)
            self.go(1, self.get(slot, 1), -1)

        def direct(self):
            self.go(2, self.get(ring(self.axis, 1), 1), 1)
            self.go(3, self.get(ring(self.axis, -1), 0), -1)

        def summed(self):
            for j, step in ((0, 1), (1, -1)):
                mine = self.get(ring(self.axis, step), j)
                self.out[j].wait_recv()
                self.go(4 + j, mine + self.rx[self.axis, j].astype(F32), step)

        def end(self):
            own0 = self.get(pos[self.axis], 0)
            own1 = self.get(pos[self.axis], 1)
            for j in (2, 3, 4, 5):
                self.out[j].wait_recv()
            rx = self.rx
            r0 = own0 + rx[self.axis, 3].astype(F32) + rx[self.axis, 4].astype(F32)
            r1 = own1 + rx[self.axis, 2].astype(F32) + rx[self.axis, 5].astype(F32)
            return r0, r1

        def drain(self):
            for c in self.out.values():
                c.wait_send()

    class Direct:
        def __init__(self, tx, rx, axis, base, get):
            self.tx, self.rx, self.axis, self.base, self.get = tx, rx, axis, base, get
            self.out = {}

        def go(self, j, step):
            axis = self.axis
            self.tx[axis, j] = self.get(ring(axis, step)).astype(BF16)
            c = remote(
                self.tx.at[axis, j], self.rx.at[axis, j],
                rs.at[axis, self.base + j], rr.at[axis, self.base + j], peer(axis, step),
            )
            c.start()
            self.out[j] = c

        def far(self):
            self.go(0, 2)

        def direct(self):
            self.go(1, 1)
            self.go(2, -1)

        def end(self):
            total = self.get(pos[self.axis])
            for j in (1, 2, 0):
                self.out[j].wait_recv()
                total = total + self.rx[self.axis, j].astype(F32)
            return total

        def drain(self):
            for c in self.out.values():
                c.wait_send()

    def get_dq(h):
        return lambda slot: dqt[h, slot] * SCALE

    def get_dkv(h):
        return lambda slot, p: dkv[h, slot, p] * (SCALE if p == 0 else 1.0)

    def get_last(h):
        def get(slot):
            rows = pl.ds(pl.multiple_of(slot * 128, 128), 128)
            return jnp.concatenate([wide[h, rows, :], wide[2 + h, rows, :]], axis=1)

        return get

    both = (0, 1)
    dq = [Direct(qtx, qrx, h, 0, get_dq(h)) for h in both]
    dk = [Reduction(ktx, krx, 1 - h, 18, get_dkv(h)) for h in both]
    wb = [Direct(btx, brx, 1 - h, 12, get_last(h)) for h in both]

    pending = some_units(
        8,
        lambda n: (
            jnp.where((n == 0) | (n > 4), 1, 0),
            jnp.where(n > 4, n - 5, 3),
            jnp.where((n == 0) | (n > 4), 3, n - 1),
        ),
        pending,
        False,
    )
    products(*pending)
    for h in both:
        dq[h].far()
    dq[0].direct()
    dq[1].direct()
    for h in both:
        dk[h].far()
    swaps = []
    for c in shares:
        c.wait_recv()
    for axis in (0, 1):
        for role in (0, 1):
            ref = lx.at[axis, role, :, :, rows, :]
            c = remote(ref, ref, ds.at[axis, role], dr.at[axis, role], sibling)
            c.start()
            swaps.append(c)
    def block(h, owner, o):
        return lat[o, owner] if h == 0 else lat[owner, o]

    def term(h, role, w, owner, o):
        near = dot(dqf[h], block(h, owner, 2 * role + o))
        return near + dot(dqg[h, role], lx[h, role, w, o])

    hands = {}
    for h in both:
        dqf[h] = dq[h].end().astype(BF16)
        for role in both:
            c = remote(
                dqf.at[h], dqg.at[h, role], hs.at[h, role], hr.at[h, role], peer(h, role_step(h, role))
            )
            c.start()
            hands[h, role] = c
    for h in both:
        dk[h].direct()
    odd = [pos[1 - h] % 2 for h in both]
    trades = {}
    for h in both:
        for role in both:
            for n, o in enumerate((odd[h], 1 - odd[h])):
                pre[h, role, n] = dot(dqf[h], block(h, ring(h, role_step(h, 1 - role)), 2 * role + o))
    for h in both:
        dk[h].summed()
    for c in swaps:
        c.wait_recv()
    for n in both:
        for h in both:
            o = odd[h] if n == 0 else 1 - odd[h]
            for role in both:
                if n == 0:
                    hands[h, role].wait_recv()
                etx[h, role, n] = (pre[h, role, n] + dot(dqg[h, role], lx[h, role, 1, o])).astype(BF16)
                c = remote(
                    etx.at[h, role, n], erx.at[h, role, n], es.at[h, role, n], er.at[h, role, n],
                    peer(h, role_step(h, 1 - role)),
                )
                c.start()
                trades[h, role, n] = c

    def place(h, slot):
        return pl.ds(pl.multiple_of(slot * 128, 128), 128)

    for h in both:
        for role in both:
            for o in both:
                part = term(h, role, 0, pos[h], o)
                wide[h, place(h, 2 * role + o), :] = part[:, 0:128]
                wide[2 + h, place(h, 2 * role + o), :] = part[:, 128:256]
    for h in both:
        wide2[pl.ds(h, T, stride=2), :] = jnp.transpose(dqf[h].astype(F32))
    qg_ref[...] = wide2[0 : 2 * T, :].astype(BF16)
    for n in both:
        for h in both:
            o = odd[h] if n == 0 else 1 - odd[h]
            for role in both:
                trades[h, role, n].wait_recv()
                got = erx[h, role, n].astype(F32)
                wide[h, place(h, 2 * role + o), :] += got[:, 0:128]
                wide[2 + h, place(h, 2 * role + o), :] += got[:, 128:256]
            if n == 0:
                wb[h].far()
            else:
                wb[h].direct()
    ends = [dk[h].end() for h in both]
    for p, ref in ((0, kg_ref), (1, vg_ref)):
        for h in both:
            wide2[pl.ds(2 * T * p + h, T, stride=2), :] = ends[h][p]
        ref[...] = wide2[2 * T * p : 2 * T * p + 2 * T, :].astype(BF16)
    for h in both:
        wg_ref[:, h * W : h * W + W] = jnp.transpose(wb[h].end())

    for c in first.values():
        c.wait_send()
    for c in second:
        c.wait_send()
    for forward in (False, True):
        z_each(names, forward, wait_send)
    for c in shares + swaps + list(hands.values()) + list(trades.values()):
        c.wait_send()
    for group in (dq, dk, wb):
        for r in group:
            r.drain()


def put_kernel(*refs):
    sems = refs[8]
    copies = [pltpu.make_async_copy(refs[n], refs[4 + n], sems.at[n]) for n in range(4)]
    for c in copies:
        c.start()
    for c in copies:
        c.wait()


def body(latents, query_heads, key_heads, value_heads, map_outputs, log_sums, out_grad, mix_lambda, norm_gain):
    rows = 2 * T
    hbm = pl.BlockSpec(memory_space=pltpu.HBM)
    vmem = pl.BlockSpec(memory_space=pltpu.VMEM)
    out_shape = (
        jax.ShapeDtypeStruct((rows, W), BF16),
        jax.ShapeDtypeStruct((rows, W), BF16),
        jax.ShapeDtypeStruct((rows, W), BF16),
        jax.ShapeDtypeStruct((T, 2 * W), F32),
    )
    outs = pl.pallas_call(
        kernel,
        out_shape=tuple(pltpu.VMEM(o.shape, o.dtype) for o in out_shape),
        in_specs=[hbm] * 9,
        out_specs=(vmem, vmem, vmem, vmem),
        scratch_shapes=[
            pltpu.VMEM((rows, W), BF16),
            pltpu.VMEM((rows, W), BF16),
            pltpu.VMEM((rows, W), BF16),
            pltpu.VMEM((2 * rows, W), BF16),
            pltpu.VMEM((2, 2, T), F32),
            pltpu.VMEM((rows, W), BF16),
            pltpu.SMEM((2,), F32),
            pltpu.VMEM((1, W), F32),
            pltpu.VMEM((4, 4, T, T), BF16),
            pltpu.VMEM((2, 2, 2, 2, T, T), BF16),
            pltpu.VMEM((2, 4, 2, T, W), BF16),
            pltpu.VMEM((2, 4, 2, T, W), BF16),
            pltpu.VMEM((2, 4, 8, T), F32),
            pltpu.VMEM((2, 4, W, T), F32),
            pltpu.VMEM((2, 4, 2, T, W), F32),
            pltpu.VMEM((3, T, T), BF16),
            pltpu.VMEM((4, rows, W), F32),
            pltpu.VMEM((4 * T, W), F32),
            pltpu.VMEM((2, W, T), BF16),
            pltpu.VMEM((2, 2, W, T), BF16),
            pltpu.VMEM((2, 3, W, T), BF16),
            pltpu.VMEM((2, 3, W, T), BF16),
            pltpu.VMEM((2, 6, T, W), BF16),
            pltpu.VMEM((2, 6, T, W), BF16),
            pltpu.VMEM((2, 2, 2, W, T), BF16),
            pltpu.VMEM((2, 2, 2, W, T), BF16),
            pltpu.VMEM((2, 3, W, T), BF16),
            pltpu.VMEM((2, 3, W, T), BF16),
            pltpu.VMEM((2, 2, 2, W, T), F32),
            pltpu.SemaphoreType.DMA((24,)),
            pltpu.SemaphoreType.DMA((2, 2, 10)),
            pltpu.SemaphoreType.DMA((2, 2, 10)),
            pltpu.SemaphoreType.DMA((2, 24)),
            pltpu.SemaphoreType.DMA((2, 24)),
            pltpu.SemaphoreType.DMA((2, 2, 2)),
            pltpu.SemaphoreType.DMA((2, 2, 2)),
            pltpu.SemaphoreType.DMA((2, 2)),
            pltpu.SemaphoreType.DMA((2, 2)),
            pltpu.SemaphoreType.DMA((2, 2)),
            pltpu.SemaphoreType.DMA((2, 2)),
            pltpu.SemaphoreType.DMA((2, 2, 2)),
            pltpu.SemaphoreType.DMA((2, 2, 2)),
        ],
        compiler_params=pltpu.CompilerParams(
            collective_id=0, has_side_effects=True, vmem_limit_bytes=VMEM_ALL
        ),
    )(
        query_heads.reshape(rows, W),
        key_heads.reshape(rows, W),
        value_heads.reshape(rows, W),
        map_outputs.reshape(2 * rows, W),
        jnp.transpose(log_sums, (1, 2, 0)),
        out_grad.reshape(rows, W),
        mix_lambda,
        norm_gain.reshape(1, W),
        latents,
    )
    qg, kg, vg, wg = pl.pallas_call(
        put_kernel,
        out_shape=out_shape,
        in_specs=[vmem] * 4,
        out_specs=(hbm, hbm, hbm, hbm),
        scratch_shapes=[pltpu.SemaphoreType.DMA((4,))],
        compiler_params=pltpu.CompilerParams(vmem_limit_bytes=1024 * 1024),
    )(*outs)
    shape = query_heads.shape
    return (qg.reshape(shape), kg.reshape(shape), vg.reshape(shape), wg)


def solution(mesh):
    placed = (
        P("sp", None),
        P("sp", "tp", None),
        P("sp", "tp", None),
        P("sp", "tp", None),
        P("sp", None, "tp", None),
        P("sp", "tp", None),
        P("sp", "tp", None),
        P("tp"),
        P(),
    )
    return jax.shard_map(
        body,
        mesh=mesh,
        in_specs=placed,
        out_specs=(P("sp", "tp", None), P("sp", "tp", None), P("sp", "tp", None), P("sp", "tp")),
        check_vma=False,
    )
```

```python
import functools

import jax
import jax.numpy as jnp
from jax import lax
from jax.experimental import pallas as pl
from jax.experimental.pallas import tpu as pltpu
from jax.sharding import PartitionSpec as P

F32 = jnp.float32
BF16 = jnp.bfloat16
EPSILON = 1e-05
LOG2E = 1.4426950408889634
SCALE = 0.125
T = 256
W = 128
VMEM_ALL = 66200000
NT = (((1,), (1,)), ((), ()))


def dot(a, b):
    return jnp.dot(a, b, preferred_element_type=F32)


def dot_nt(a, b):
    return lax.dot_general(a, b, NT, preferred_element_type=F32)


def kernel(
    q_hbm, k_hbm, v_hbm, mo_hbm, lse_hbm, og_hbm, lam_hbm, gain_hbm, lat_hbm,
    qg_ref, kg_ref, vg_ref, wg_ref,
    q_in, k_in, v_in, mo_in, lse_in, og_in, lam_in, gain_in,
    lat, lx, qdo, kv, st, dqt, dkv, wds, wide, wide2, dqf, dqg,
    qtx, qrx, ktx, krx, etx, erx, btx, brx, pre,
    in_sem, gs, gr, rs, rr, ls, lr, ds, dr, hs, hr, es, er,
):
    sp = lax.axis_index("sp")
    tp = lax.axis_index("tp")
    z = sp // 4
    y = sp % 4
    pos = (y, z)

    def ring(axis, step):
        return lax.rem(pos[axis] + step + 4, 4)

    def peer(axis, step):
        moved = ring(axis, step)
        return (z * 4 + moved if axis == 0 else moved * 4 + y, tp)

    def remote(src, dst, send, recv, device):
        return pltpu.make_async_remote_copy(
            src_ref=src, dst_ref=dst, send_sem=send, recv_sem=recv,
            device_id=device, device_id_type=pl.DeviceIdType.MESH,
        )

    def role_step(axis, role):
        sign = 1 - 2 * (pos[axis] % 2)
        return sign if role == 0 else -sign

    core = tp % 2
    sibling = (sp, tp + 1 - 2 * core)
    barrier = pltpu.get_barrier_semaphore()
    pl.semaphore_signal(barrier, inc=1, device_id=sibling, device_id_type=pl.DeviceIdType.MESH)
    for axis in (0, 1):
        for step in (1, -1, 2):
            pl.semaphore_signal(
                barrier, inc=1, device_id=peer(axis, step), device_id_type=pl.DeviceIdType.MESH
            )
    sources = (q_hbm, k_hbm, v_hbm, og_hbm, mo_hbm, lse_hbm, lam_hbm, gain_hbm)
    targets = (q_in, k_in, v_in, og_in, mo_in, lse_in, lam_in, gain_in)
    loads = [pltpu.make_async_copy(a, b, in_sem.at[n]) for n, (a, b) in enumerate(zip(sources, targets))]
    loads += [
        pltpu.make_async_copy(lat_hbm.at[:, n * T : n * T + T], lat.at[n // 4, n % 4], in_sem.at[8 + n])
        for n in range(16)
    ]
    for c in loads:
        c.start()

    qpos = (y, z)
    kpos = (z, y)
    qh = (0, 1)
    kh = (1, 0)
    first = {}

    def item(axis, name, slot):
        if name == "q":
            return qdo.at[qh[axis], slot, 0]
        if name == "do":
            return qdo.at[qh[axis], slot, 1]
        if name == "st":
            return st.at[qh[axis], slot]
        if name == "k":
            return kv.at[kh[axis], slot, 0]
        return kv.at[kh[axis], slot, 1]

    names = ("q", "k", "v", "do", "st")

    def gather_copy(axis, d, name, slot, forward):
        n = names.index(name) + (5 if forward else 0)
        ref = item(axis, name, slot)
        step = 1 if d == 0 else -1
        return remote(ref, ref, gs.at[axis, d, n], gr.at[axis, d, n], peer(axis, step))

    ups = ("k", "v")
    downs = ("q", "do", "st")

    def z_each(some, forward, do_it):
        if forward:
            middle = (z == 1) | (z == 2)
            cases = ((0, middle, ups, -1), (1, middle, downs, 1))
        else:
            cases = ((0, z < 3, ups, 0), (0, z == 3, downs, 0), (1, z > 0, downs, 0), (1, z == 0, ups, 0))
        for d, wanted, group, shift in cases:
            mine = [name for name in some if name in group]
            if mine:
                @pl.when(wanted)
                def _():
                    for name in mine:
                        do_it(gather_copy(1, d, name, ring(1, shift), forward))

    def z_arrived(some, forward):
        if forward:
            cases = ((0, z >= 2, ups, 2), (1, z < 2, downs, 2))
        else:
            cases = ((0, z > 0, ups, -1), (0, z == 0, downs, -1), (1, z < 3, downs, 1), (1, z == 3, ups, 1))
        for d, wanted, group, shift in cases:
            mine = [name for name in some if name in group]
            if mine:
                @pl.when(wanted)
                def _():
                    for name in mine:
                        gather_copy(1, d, name, ring(1, shift), forward).wait_recv()

    def start(c):
        c.start()

    def wait_send(c):
        c.wait_send()

    def send_y(*some):
        for d, name in some:
            c = gather_copy(0, d, name, y, False)
            c.start()
            first[d, name] = c

    for n, (name, ref) in enumerate((("q", q_in), ("k", k_in), ("v", v_in))):
        loads[n].wait()
        wide[n] = ref[...].astype(F32)
        for h in (0, 1):
            part = wide[n, pl.ds(h, T, stride=2), :].astype(BF16)
            if n == 0:
                qdo[h, qpos[h], 0] = part
            else:
                kv[h, kpos[h], n - 1] = part
        if n == 0:
            pl.semaphore_wait(barrier, 7)
        send_y(*(((1, "v"), (0, "v")) if name == "v" else ((0, name),)))
        z_each((name,), False, start)

    for c in loads[3:8]:
        c.wait()
    wide[3] = og_in[...].astype(F32)
    wide2[...] = mo_in[...].astype(F32)
    gain = gain_in[...]
    for h in (0, 1):
        lam = lam_in[h]
        m1 = wide2[pl.ds(h, T, stride=4), :]
        m2 = wide2[pl.ds(2 + h, T, stride=4), :]
        comb = m1 - lam * m2
        inv = lax.rsqrt(jnp.mean(comb * comb, axis=-1, keepdims=True) + EPSILON)
        wtd = gain * wide[3, pl.ds(h, T, stride=2), :]
        cross = jnp.mean(comb * wtd, axis=-1, keepdims=True)
        grad = (inv * wtd - inv * inv * inv * comb * cross).astype(BF16)
        qdo[h, qpos[h], 1] = grad
        gf = grad.astype(F32)
        r1 = jnp.sum(jnp.transpose(gf * m1), axis=0, keepdims=True)
        r2 = jnp.sum(jnp.transpose(gf * m2), axis=0, keepdims=True)
        lam_row = jnp.full((1, T), lam, F32)
        st[h, qpos[h], 0:1] = lse_in[h, 0:1, :] * LOG2E
        st[h, qpos[h], 1:2] = (lse_in[h, 1:2, :] - jnp.log(lam_row)) * LOG2E
        st[h, qpos[h], 2:3] = r1
        st[h, qpos[h], 3:4] = r2
        st[h, qpos[h], 4:8] = jnp.zeros((4, T), F32)
    send_y((1, "do"), (1, "st"))
    z_each(("do",), False, start)
    z_each(("st",), False, start)
    send_y((1, "q"), (1, "k"), (0, "do"), (0, "st"))

    dqt[...] = jnp.zeros_like(dqt)
    dkv[...] = jnp.zeros_like(dkv)

    lane = lax.broadcasted_iota(jnp.int32, (T, W), 1)

    def split_queries(h, qs):
        q = qdo[h, qs, 0]
        zero = jnp.zeros_like(q)
        return jnp.where(lane < 64, q, zero), jnp.where(lane < 64, zero, -q)

    def scores(h, qs, ks, masked):
        q1, q2 = split_queries(h, qs)
        do = qdo[h, qs, 1]
        half = T // 2
        for c in (0, half):
            k = kv[h, ks, 0, c : c + half]
            v = kv[h, ks, 1, c : c + half]
            s1 = dot_nt(k, q1)
            s2 = dot_nt(k, q2)
            dp = dot_nt(v, do)
            p1 = jnp.exp2(s1 * (SCALE * LOG2E) - st[h, qs, 0:1])
            p2 = jnp.exp2(s2 * (-SCALE * LOG2E) - st[h, qs, 1:2])
            if masked:
                rows = lax.broadcasted_iota(jnp.int32, (half, T), 0) + c
                cols = lax.broadcasted_iota(jnp.int32, (half, T), 1)
                keep = rows <= cols
                p1 = jnp.where(keep, p1, 0.0)
                p2 = jnp.where(keep, p2, 0.0)
            wds[0, c : c + half] = (p1 - p2).astype(BF16)
            wds[1, c : c + half] = (p1 * (dp - st[h, qs, 2:3])).astype(BF16)
            wds[2, c : c + half] = (p2 * (dp - st[h, qs, 3:4])).astype(BF16)

    def products(h, qs, ks):
        q1, q2 = split_queries(h, qs)
        w, d1, d2 = wds[0], wds[1], wds[2]
        kt = jnp.transpose(kv[h, ks, 0])
        dqt[h, qs, 0:64] += dot(kt[0:64], d1)
        dqt[h, qs, 64:128] -= dot(kt[64:128], d2)
        dkv[h, ks, 0] += dot(d1, q1) + dot(d2, q2)
        dkv[h, ks, 1] += dot(w, qdo[h, qs, 1])

    def maybe_unit(h, i, j, before):
        qo = jnp.where(i < 2, i, 5 - i)
        ko = jnp.where(j < 2, j, 5 - j)
        qbase = jnp.where(h == 0, y, z)
        kbase = jnp.where(h == 0, z, y)
        qs = (qbase + qo) % 4
        ks = (kbase + ko) % 4
        q_block = jnp.where(h == 0, z * 4 + qs, qs * 4 + y)
        k_block = jnp.where(h == 0, ks * 4 + y, z * 4 + ks)
        wanted = k_block < q_block

        @pl.when(wanted)
        def _():
            products(*before)
            scores(h, qs, ks, False)

        return tuple(jnp.where(wanted, a, b) for a, b in zip((h, qs, ks), before))

    def some_units(count, which, before, fresh):
        if fresh:
            wds[...] = jnp.zeros_like(wds)

        def step(n, carry):
            return maybe_unit(*which(n), carry)

        return lax.fori_loop(0, count, step, before)

    scores(0, y, z, True)
    products(0, y, z)
    scores(1, z, y, True)
    pending = (jnp.int32(1), z, y)

    second = []
    rows = pl.ds(pl.multiple_of(core * 128, 128), 128)
    shares = []

    def share(axis):
        for role in (0, 1):
            step = role_step(axis, role)
            for w, owner in enumerate((ring(axis, step), ring(axis, 2))):
                some = slice(2 * role, 2 * role + 2)
                src = lat.at[some, owner, rows, :] if axis == 0 else lat.at[owner, some, rows, :]
                c = remote(
                    src, lx.at[axis, role, w, :, rows, :], ls.at[axis, role, w], lr.at[axis, role, w],
                    peer(axis, step),
                )
                c.start()
                shares.append(c)

    for d, name in ((0, "q"), (1, "v"), (0, "k"), (1, "do"), (1, "st")):
        first[d, name].wait_recv()
        c = gather_copy(0, d, name, ring(0, -1 if d == 0 else 1), True)
        c.start()
        second.append(c)
    for some in (("q", "k"), ("v",), ("do", "st")):
        z_arrived(some, False)
        z_each(some, True, start)
    for c in loads[8:]:
        c.wait()
    share(1)
    pending = some_units(
        4, lambda n: (n // 2, jnp.where(n < 2, 0, n - 1), jnp.where(n < 2, n + 1, 0)), pending, False
    )
    for d, name in ((1, "q"), (1, "k"), (0, "v"), (0, "do"), (0, "st")):
        first[d, name].wait_recv()

    share(0)

    pending = some_units(
        12,
        lambda n: (
            n // 6,
            jnp.where(n < 6, n // 3 + 1, n % 3),
            jnp.where(n < 6, n % 3, (n - 6) // 3 + 1),
        ),
        pending,
        False,
    )
    z_arrived(names, True)
    pending = some_units(
        6, lambda n: (n // 3, jnp.where(n < 3, n, 3), jnp.where(n < 3, 3, n - 3)), pending, False
    )
    for c in second:
        c.wait_recv()

    class Reduction:
        def __init__(self, tx, rx, axis, base, get):
            self.tx, self.rx, self.axis, self.base, self.get = tx, rx, axis, base, get
            self.out = {}

        def go(self, j, value, step):
            axis = self.axis
            self.tx[axis, j] = value.astype(BF16)
            c = remote(
                self.tx.at[axis, j], self.rx.at[axis, j],
                rs.at[axis, self.base + j], rr.at[axis, self.base + j], peer(axis, step),
            )
            c.start()
            self.out[j] = c

        def far(self):
            slot = ring(self.axis, 2)
            self.go(0, self.get(slot, 0), 1)
            self.go(1, self.get(slot, 1), -1)

        def direct(self):
            self.go(2, self.get(ring(self.axis, 1), 1), 1)
            self.go(3, self.get(ring(self.axis, -1), 0), -1)

        def summed(self):
            for j, step in ((0, 1), (1, -1)):
                mine = self.get(ring(self.axis, step), j)
                self.out[j].wait_recv()
                self.go(4 + j, mine + self.rx[self.axis, j].astype(F32), step)

        def end(self):
            own0 = self.get(pos[self.axis], 0)
            own1 = self.get(pos[self.axis], 1)
            for j in (2, 3, 4, 5):
                self.out[j].wait_recv()
            rx = self.rx
            r0 = own0 + rx[self.axis, 3].astype(F32) + rx[self.axis, 4].astype(F32)
            r1 = own1 + rx[self.axis, 2].astype(F32) + rx[self.axis, 5].astype(F32)
            return r0, r1

        def drain(self):
            for c in self.out.values():
                c.wait_send()

    class Direct:
        def __init__(self, tx, rx, axis, base, get):
            self.tx, self.rx, self.axis, self.base, self.get = tx, rx, axis, base, get
            self.out = {}

        def go(self, j, step):
            axis = self.axis
            self.tx[axis, j] = self.get(ring(axis, step)).astype(BF16)
            c = remote(
                self.tx.at[axis, j], self.rx.at[axis, j],
                rs.at[axis, self.base + j], rr.at[axis, self.base + j], peer(axis, step),
            )
            c.start()
            self.out[j] = c

        def far(self):
            self.go(0, 2)

        def direct(self):
            self.go(1, 1)
            self.go(2, -1)

        def end(self):
            total = self.get(pos[self.axis])
            for j in (1, 2, 0):
                self.out[j].wait_recv()
                total = total + self.rx[self.axis, j].astype(F32)
            return total

        def drain(self):
            for c in self.out.values():
                c.wait_send()

    def get_dq(h):
        return lambda slot: dqt[h, slot] * SCALE

    def get_dkv(h):
        return lambda slot, p: dkv[h, slot, p] * (SCALE if p == 0 else 1.0)

    def get_last(h):
        def get(slot):
            rows = pl.ds(pl.multiple_of(slot * 128, 128), 128)
            return jnp.concatenate([wide[h, rows, :], wide[2 + h, rows, :]], axis=1)

        return get

    both = (0, 1)
    dq = [Direct(qtx, qrx, h, 0, get_dq(h)) for h in both]
    dk = [Reduction(ktx, krx, 1 - h, 18, get_dkv(h)) for h in both]
    wb = [Direct(btx, brx, 1 - h, 12, get_last(h)) for h in both]

    pending = some_units(
        8,
        lambda n: (
            jnp.where((n == 0) | (n > 4), 1, 0),
            jnp.where(n > 4, n - 5, 3),
            jnp.where((n == 0) | (n > 4), 3, n - 1),
        ),
        pending,
        False,
    )
    products(*pending)
    for h in both:
        dq[h].far()
    dq[0].direct()
    dq[1].direct()
    for h in both:
        dk[h].far()
    swaps = []
    for c in shares:
        c.wait_recv()
    for axis in (0, 1):
        for role in (0, 1):
            ref = lx.at[axis, role, :, :, rows, :]
            c = remote(ref, ref, ds.at[axis, role], dr.at[axis, role], sibling)
            c.start()
            swaps.append(c)
    def block(h, owner, o):
        return lat[o, owner] if h == 0 else lat[owner, o]

    def term(h, role, w, owner, o):
        near = dot(dqf[h], block(h, owner, 2 * role + o))
        return near + dot(dqg[h, role], lx[h, role, w, o])

    hands = {}
    for h in both:
        dqf[h] = dq[h].end().astype(BF16)
        for role in both:
            c = remote(
                dqf.at[h], dqg.at[h, role], hs.at[h, role], hr.at[h, role], peer(h, role_step(h, role))
            )
            c.start()
            hands[h, role] = c
    odd = [pos[1 - h] % 2 for h in both]
    trades = {}
    for h in both:
        for role in both:
            for n, o in enumerate((odd[h], 1 - odd[h])):
                pre[h, role, n] = dot(dqf[h], block(h, ring(h, role_step(h, 1 - role)), 2 * role + o))
    for h in both:
        dk[h].summed()
    for c in swaps:
        c.wait_recv()
    for n in both:
        for h in both:
            o = odd[h] if n == 0 else 1 - odd[h]
            for role in both:
                if n == 0:
                    hands[h, role].wait_recv()
                etx[h, role, n] = (pre[h, role, n] + dot(dqg[h, role], lx[h, role, 1, o])).astype(BF16)
                c = remote(
                    etx.at[h, role, n], erx.at[h, role, n], es.at[h, role, n], er.at[h, role, n],
                    peer(h, role_step(h, 1 - role)),
                )
                c.start()
                trades[h, role, n] = c

    for h in both:
        dk[h].direct()

    def place(h, slot):
        return pl.ds(pl.multiple_of(slot * 128, 128), 128)

    for h in both:
        for role in both:
            for o in both:
                part = term(h, role, 0, pos[h], o)
                wide[h, place(h, 2 * role + o), :] = part[:, 0:128]
                wide[2 + h, place(h, 2 * role + o), :] = part[:, 128:256]
    for h in both:
        wide2[pl.ds(h, T, stride=2), :] = jnp.transpose(dqf[h].astype(F32))
    qg_ref[...] = wide2[0 : 2 * T, :].astype(BF16)
    for n in both:
        for h in both:
            o = odd[h] if n == 0 else 1 - odd[h]
            for role in both:
                trades[h, role, n].wait_recv()
                got = erx[h, role, n].astype(F32)
                wide[h, place(h, 2 * role + o), :] += got[:, 0:128]
                wide[2 + h, place(h, 2 * role + o), :] += got[:, 128:256]
            if n == 0:
                wb[h].far()
            else:
                wb[h].direct()
    ends = [dk[h].end() for h in both]
    for p, ref in ((0, kg_ref), (1, vg_ref)):
        for h in both:
            wide2[pl.ds(2 * T * p + h, T, stride=2), :] = ends[h][p]
        ref[...] = wide2[2 * T * p : 2 * T * p + 2 * T, :].astype(BF16)
    for h in both:
        wg_ref[:, h * W : h * W + W] = jnp.transpose(wb[h].end())

    for c in first.values():
        c.wait_send()
    for c in second:
        c.wait_send()
    for forward in (False, True):
        z_each(names, forward, wait_send)
    for c in shares + swaps + list(hands.values()) + list(trades.values()):
        c.wait_send()
    for group in (dq, dk, wb):
        for r in group:
            r.drain()


def put_kernel(*refs):
    sems = refs[8]
    copies = [pltpu.make_async_copy(refs[n], refs[4 + n], sems.at[n]) for n in range(4)]
    for c in copies:
        c.start()
    for c in copies:
        c.wait()


def body(latents, query_heads, key_heads, value_heads, map_outputs, log_sums, out_grad, mix_lambda, norm_gain):
    rows = 2 * T
    hbm = pl.BlockSpec(memory_space=pltpu.HBM)
    vmem = pl.BlockSpec(memory_space=pltpu.VMEM)
    out_shape = (
        jax.ShapeDtypeStruct((rows, W), BF16),
        jax.ShapeDtypeStruct((rows, W), BF16),
        jax.ShapeDtypeStruct((rows, W), BF16),
        jax.ShapeDtypeStruct((T, 2 * W), F32),
    )
    outs = pl.pallas_call(
        kernel,
        out_shape=tuple(pltpu.VMEM(o.shape, o.dtype) for o in out_shape),
        in_specs=[hbm] * 9,
        out_specs=(vmem, vmem, vmem, vmem),
        scratch_shapes=[
            pltpu.VMEM((rows, W), BF16),
            pltpu.VMEM((rows, W), BF16),
            pltpu.VMEM((rows, W), BF16),
            pltpu.VMEM((2 * rows, W), BF16),
            pltpu.VMEM((2, 2, T), F32),
            pltpu.VMEM((rows, W), BF16),
            pltpu.SMEM((2,), F32),
            pltpu.VMEM((1, W), F32),
            pltpu.VMEM((4, 4, T, T), BF16),
            pltpu.VMEM((2, 2, 2, 2, T, T), BF16),
            pltpu.VMEM((2, 4, 2, T, W), BF16),
            pltpu.VMEM((2, 4, 2, T, W), BF16),
            pltpu.VMEM((2, 4, 8, T), F32),
            pltpu.VMEM((2, 4, W, T), F32),
            pltpu.VMEM((2, 4, 2, T, W), F32),
            pltpu.VMEM((3, T, T), BF16),
            pltpu.VMEM((4, rows, W), F32),
            pltpu.VMEM((4 * T, W), F32),
            pltpu.VMEM((2, W, T), BF16),
            pltpu.VMEM((2, 2, W, T), BF16),
            pltpu.VMEM((2, 3, W, T), BF16),
            pltpu.VMEM((2, 3, W, T), BF16),
            pltpu.VMEM((2, 6, T, W), BF16),
            pltpu.VMEM((2, 6, T, W), BF16),
            pltpu.VMEM((2, 2, 2, W, T), BF16),
            pltpu.VMEM((2, 2, 2, W, T), BF16),
            pltpu.VMEM((2, 3, W, T), BF16),
            pltpu.VMEM((2, 3, W, T), BF16),
            pltpu.VMEM((2, 2, 2, W, T), F32),
            pltpu.SemaphoreType.DMA((24,)),
            pltpu.SemaphoreType.DMA((2, 2, 10)),
            pltpu.SemaphoreType.DMA((2, 2, 10)),
            pltpu.SemaphoreType.DMA((2, 24)),
            pltpu.SemaphoreType.DMA((2, 24)),
            pltpu.SemaphoreType.DMA((2, 2, 2)),
            pltpu.SemaphoreType.DMA((2, 2, 2)),
            pltpu.SemaphoreType.DMA((2, 2)),
            pltpu.SemaphoreType.DMA((2, 2)),
            pltpu.SemaphoreType.DMA((2, 2)),
            pltpu.SemaphoreType.DMA((2, 2)),
            pltpu.SemaphoreType.DMA((2, 2, 2)),
            pltpu.SemaphoreType.DMA((2, 2, 2)),
        ],
        compiler_params=pltpu.CompilerParams(
            collective_id=0, has_side_effects=True, vmem_limit_bytes=VMEM_ALL
        ),
    )(
        query_heads.reshape(rows, W),
        key_heads.reshape(rows, W),
        value_heads.reshape(rows, W),
        map_outputs.reshape(2 * rows, W),
        jnp.transpose(log_sums, (1, 2, 0)),
        out_grad.reshape(rows, W),
        mix_lambda,
        norm_gain.reshape(1, W),
        latents,
    )
    qg, kg, vg, wg = pl.pallas_call(
        put_kernel,
        out_shape=out_shape,
        in_specs=[vmem] * 4,
        out_specs=(hbm, hbm, hbm, hbm),
        scratch_shapes=[pltpu.SemaphoreType.DMA((4,))],
        compiler_params=pltpu.CompilerParams(vmem_limit_bytes=1024 * 1024),
    )(*outs)
    shape = query_heads.shape
    return (qg.reshape(shape), kg.reshape(shape), vg.reshape(shape), wg)


def solution(mesh):
    placed = (
        P("sp", None),
        P("sp", "tp", None),
        P("sp", "tp", None),
        P("sp", "tp", None),
        P("sp", None, "tp", None),
        P("sp", "tp", None),
        P("sp", "tp", None),
        P("tp"),
        P(),
    )
    return jax.shard_map(
        body,
        mesh=mesh,
        in_specs=placed,
        out_specs=(P("sp", "tp", None), P("sp", "tp", None), P("sp", "tp", None), P("sp", "tp")),
        check_vma=False,
    )
```
